512 devices in a mesh: sp: 64 (over z, y), tp: 8 (over x, core).
Axes of the slice: x: 4, y: 8, z: 8, core: 2. Of those that a mesh axis runs over, the one named last changes fastest.
Arguments:
- hidden_in: bfloat16 [24576, 2048], P('sp'), may hold values from -6 to 6
- drive: bfloat16 [24576, 1024], P('sp', 'tp'), may hold values from -24 to 24
- wide_poles: float32 [2, 32, 64], P(None, 'tp'), may hold values from -2 to 256, as said below
- narrow_poles: float32 [2, 32, 32], P(None, 'tp'), may hold values from -2 to 128, as said below
- log_step: float32 [32, 2], P('tp'), may hold values from -3.912 to -2.526
- forget: float32 [32, 2, 24576], P('tp', None, 'sp'), may hold values from 0 to 2
- wide_input: bfloat16 [2, 32, 64, 16], P(None, 'tp'), may hold values from -1 to 1
- narrow_input: bfloat16 [2, 32, 32, 16], P(None, 'tp'), may hold values from -1 to 1
- wide_output: bfloat16 [2, 32, 16, 64], P(None, 'tp'), may hold values from -0.5 to 0.5
- narrow_output: bfloat16 [2, 32, 16, 32], P(None, 'tp'), may hold values from -0.75 to 0.75
- skip: float32 [1024], P('tp'), may hold values from -4 to 4
- mix_gain: float32 [1024], P('tp'), may hold values from 0.1 to 1.9
- out_weight: bfloat16 [1024, 2048], P('tp'), may hold values from -0.1875 to 0.1875
- mlp_gain: float32 [2048], replicated, may hold values from 0.1 to 1.9
- up_weight: bfloat16 [2048, 8192], P('sp', 'tp'), may hold values from -0.125 to 0.125
- down_weight: bfloat16 [2048, 8192], P('sp', 'tp'), may hold values from -0.0625 to 0.0625
Outputs:
- hidden_out: bfloat16 [24576, 2048], P('sp')
The draws below stay inside these ranges and needn't reach their ends.
Inputs may be any that keep to these rules, and one draw needn't show every extreme that they name: `wide_poles`: entry 0 holds real parts, each at most -1 / 24576; entry 1 holds imaginary parts. `narrow_poles`: entry 0 holds real parts, each at most -1 / 24576; entry 1 holds imaginary parts.
All inputs are finite; a program needn't handle non-finite values.
Results may differ from the reference program's by a relative error of at most 0.02.
Values may be sent and summed in bfloat16 or wider, within the bound.
A program may use at most 64 MiB of HBM per device.

```python
import math
import jax
import jax.numpy as jnp
from jax import lax

D = 2048
FF = 8192
PAIRS = 32
GROUP = 16
SW = 64
SN = 32
TOK_DEV = 384
TOKEN_POSITIONS = 24576
CHANNELS = 1024
N_TP = 8


def pole_draw(key, state_len):
    random_subkeys = jax.random.split(key, 4)
    slow_share = 0.5
    slow_mask = jax.random.uniform(random_subkeys[0], (PAIRS, 1), jnp.float32) < slow_share
    fast_real = -jax.random.uniform(random_subkeys[1], (PAIRS, state_len), jnp.float32, 0.3, 1.6)
    slow_real = -jax.random.uniform(random_subkeys[2], (PAIRS, state_len), jnp.float32, 0.05, 0.15) / (0.05 * TOKEN_POSITIONS)
    real_part = jnp.where(slow_mask, slow_real, fast_real)
    imag_part = math.pi * jnp.arange(state_len, dtype=jnp.float32)[None, :] + jax.random.uniform(random_subkeys[3], (PAIRS, state_len), jnp.float32, -0.5, 0.5)
    return jnp.stack([real_part, imag_part])


def draw_wide_poles(key, part):
    return pole_draw(jax.random.fold_in(key, 11), SW)


def draw_narrow_poles(key, part):
    return pole_draw(jax.random.fold_in(key, 12), SN)


def draw_forget(key, part):
    random_subkeys = jax.random.split(key, 5)
    devices_along = TOKEN_POSITIONS // TOK_DEV
    parity = jax.random.randint(random_subkeys[0], (), 0, 2)
    parity_sign = jnp.where((jnp.arange(devices_along) + parity) % 2 == 0, 1.0, -1.0)
    block_level = jnp.exp(math.log(2.0) * parity_sign * jax.random.uniform(random_subkeys[1], (devices_along,), jnp.float32, 0.5, 1.0))
    per_position = jnp.repeat(block_level, TOK_DEV, total_repeat_length=TOKEN_POSITIONS)
    rough_low = 0.3
    rough_high = 1.7
    level_scale = 1.0
    roughness = jax.random.uniform(random_subkeys[2], (PAIRS, 2, TOKEN_POSITIONS), jnp.float32, rough_low, rough_high)
    baseline_level = level_scale / TOKEN_POSITIONS * per_position[None, None, :] * roughness
    spike_position = jax.random.randint(random_subkeys[3], (3,), 0, TOKEN_POSITIONS)
    spike_amount = jax.random.uniform(random_subkeys[4], (3,), jnp.float32, 0.22, 0.3)
    spike_signal = jnp.sum((jnp.arange(TOKEN_POSITIONS)[None, :] == spike_position[:, None]).astype(jnp.float32) * spike_amount[:, None], axis=0)
    return baseline_level + spike_signal[None, None, :]


def draw_drive(key, part):
    random_subkeys = jax.random.split(key, 3)
    columns = jnp.arange(CHANNELS, dtype=jnp.float32) / CHANNELS
    column_scale = jnp.exp(math.log(0.5) + math.log(6.0) * columns + jax.random.uniform(random_subkeys[0], (CHANNELS,), jnp.float32, -0.35, 0.35))
    row_scale = jnp.exp(jax.random.uniform(random_subkeys[1], (TOKEN_POSITIONS, 1), jnp.float32, math.log(0.3), math.log(3.2)))
    values = jax.random.normal(random_subkeys[2], (TOKEN_POSITIONS, CHANNELS), jnp.float32)
    return jnp.clip(values * row_scale * column_scale[None, :], -24.0, 24.0).astype(jnp.bfloat16)


def level_of(rng, dims, pieces, smallest, high):
    factor_of, own = 1.0, jax.random.fold_in(rng, 6)
    for dim, shards_of in pieces:
        steps = jnp.exp(jax.random.uniform(jax.random.fold_in(own, dim), (shards_of,), jnp.float32, smallest / len(pieces), high / len(pieces)))
        factor_of = factor_of * jnp.repeat(steps, dims[dim] // shards_of).reshape([-1 if axis == dim else 1 for axis in range(len(dims))])
    return factor_of


def normal_values(own_key, shape, width, limit, cuts=(), kind=jnp.bfloat16):
    drawn = jax.random.normal(own_key, shape, jnp.float32) * width
    if len(cuts) > 0:
        drawn = level_of(own_key, shape, cuts, -0.22, 0.18) * drawn
    return jnp.clip(drawn, min=-limit, max=limit).astype(kind)


def setup_inputs(seed: int = 0) -> dict:
    arg_keys = jax.random.split(jax.random.key(seed), 17)
    return {
        "hidden_in": normal_values(arg_keys[0], (TOKEN_POSITIONS, D), 1.0, 6.0, ((0, 64),)),
        "drive": draw_drive(jax.random.fold_in(arg_keys[16], 71), 0),
        "wide_poles": draw_wide_poles(jax.random.fold_in(arg_keys[16], 71), 0),
        "narrow_poles": draw_narrow_poles(jax.random.fold_in(arg_keys[16], 71), 0),
        "log_step": jnp.clip(-3.912 + 1.3859999 * jax.random.uniform(arg_keys[4], (PAIRS, 2), jnp.float32) ** level_of(arg_keys[4], (PAIRS, 2), ((0, 8),), -0.2, 0.2), -3.912, -2.526),
        "forget": draw_forget(jax.random.fold_in(arg_keys[16], 71), 0),
        "wide_input": normal_values(arg_keys[6], (2, PAIRS, SW, GROUP), (2 * GROUP) ** -0.5, 1.0, ((1, 8),)),
        "narrow_input": normal_values(arg_keys[7], (2, PAIRS, SN, GROUP), (2 * GROUP) ** -0.5, 1.0, ((1, 8),)),
        "wide_output": normal_values(arg_keys[8], (2, PAIRS, GROUP, SW), (2 * SW) ** -0.5, 0.5, ((1, 8),)),
        "narrow_output": normal_values(arg_keys[9], (2, PAIRS, GROUP, SN), (2 * SN) ** -0.5, 0.75, ((1, 8),)),
        "skip": normal_values(arg_keys[10], (CHANNELS,), 1.0, 4.0, ((0, 8),), jnp.float32),
        "mix_gain": jnp.clip(1.0 + 0.18 * jax.random.normal(arg_keys[11], (CHANNELS,), jnp.float32), 0.1, 1.9),
        "out_weight": normal_values(arg_keys[12], (CHANNELS, D), CHANNELS ** -0.5, 0.1875, ((0, 8),)),
        "mlp_gain": jnp.clip(1.0 + 0.18 * jax.random.normal(arg_keys[13], (D,), jnp.float32), 0.1, 1.9),
        "up_weight": normal_values(arg_keys[14], (D, FF), D ** -0.5, 0.125, ((0, 64), (1, 8))),
        "down_weight": normal_values(arg_keys[15], (D, FF), FF ** -0.5, 0.0625, ((0, 64), (1, 8))),
    }


epsilon = 1e-06

def combine(earlier, later):
    return (later[0] * earlier[0] - later[1] * earlier[1], later[0] * earlier[1] + later[1] * earlier[0], later[0] * earlier[2] - later[1] * earlier[3] + later[2], later[0] * earlier[3] + later[1] * earlier[2] + later[3])

def discretize(pole_pair, log_rate):
    step_size = jnp.exp(log_rate)[:, None]
    growth = pole_pair[0] * step_size
    angle = pole_pair[1] * step_size
    rise_real = jnp.expm1(growth) * jnp.cos(angle) - 2.0 * jnp.sin(0.5 * angle) ** 2
    rise_imag = jnp.exp(growth) * jnp.sin(angle)
    denominator = pole_pair[0] ** 2 + pole_pair[1] ** 2
    coef_real = (rise_real * pole_pair[0] + rise_imag * pole_pair[1]) / denominator
    coef_imag = (rise_imag * pole_pair[0] - rise_real * pole_pair[1]) / denominator
    return (growth, angle, coef_real, coef_imag)

def kind_states(signal_rows, decay_rows, terms, in_weight):
    growth, angle, coef_real, coef_imag = terms
    drive_real = jnp.einsum('rpg,psg->rps', signal_rows, in_weight[0].astype(jnp.float32))
    drive_imag = jnp.einsum('rpg,psg->rps', signal_rows, in_weight[1].astype(jnp.float32))
    push_real = coef_real * drive_real - coef_imag * drive_imag
    push_imag = coef_real * drive_imag + coef_imag * drive_real
    spike_magnitude = jnp.exp(growth[None] - decay_rows[:, :, None])
    return lax.associative_scan(combine, (spike_magnitude * jnp.cos(angle)[None], spike_magnitude * jnp.sin(angle)[None], push_real, push_imag), axis=0)

def read_out(state_real, state_imag, out_kind):
    first = jnp.einsum('rps,pgs->rpg', state_real, out_kind[0].astype(jnp.float32), precision=lax.Precision.HIGHEST)
    second = jnp.einsum('rps,pgs->rpg', state_imag, out_kind[1].astype(jnp.float32), precision=lax.Precision.HIGHEST)
    return first - second

def row_norm(rows_in, gain):
    values = rows_in.astype(jnp.float32)
    return (values * lax.rsqrt(lax.optimization_barrier(jnp.mean(values * values, axis=1, keepdims=True)) + epsilon) * gain).astype(jnp.bfloat16)

def reference(hidden_in, drive, wide_poles, narrow_poles, log_step, forget, wide_input, narrow_input, wide_output, narrow_output, skip, mix_gain, out_weight, mlp_gain, up_weight, down_weight):
    block_len = math.gcd(TOKEN_POSITIONS, 512)
    block_count = TOKEN_POSITIONS // block_len
    signal = drive.astype(jnp.float32).reshape(block_count, block_len, PAIRS, 2, GROUP)
    decay_all = jnp.transpose(forget, (2, 0, 1)).reshape(block_count, block_len, PAIRS, 2)
    kinds = ((wide_poles, wide_input, wide_output), (narrow_poles, narrow_input, narrow_output))
    responses = []
    for kind_index in range(2):
        pole_pair, in_weight, out_kind = kinds[kind_index]
        terms = discretize(pole_pair, log_step[:, kind_index])

        def advance(carried, block_inputs):
            cum_real, cum_imag, local_real, local_imag = kind_states(block_inputs[0], block_inputs[1], terms, in_weight)
            state_real = local_real + cum_real * carried[0][None] - cum_imag * carried[1][None]
            state_imag = local_imag + cum_real * carried[1][None] + cum_imag * carried[0][None]
            return ((state_real[-1], state_imag[-1]), read_out(state_real, state_imag, out_kind))
        initial = (jnp.zeros(pole_pair.shape[1:], jnp.float32), jnp.zeros(pole_pair.shape[1:], jnp.float32))
        _, block_outputs = lax.scan(advance, initial, (signal[:, :, :, kind_index], decay_all[:, :, :, kind_index]))
        responses.append(block_outputs.reshape(TOKEN_POSITIONS, PAIRS, GROUP))
    response = jnp.stack(responses, axis=2).reshape(TOKEN_POSITIONS, CHANNELS) + skip[None, :] * drive.astype(jnp.float32)
    active = jax.nn.gelu(response, approximate=False)
    mixed = (active * lax.rsqrt(lax.optimization_barrier(jnp.mean(active * active, axis=1, keepdims=True)) + epsilon) * mix_gain).astype(jnp.bfloat16)
    shard_width = CHANNELS // N_TP
    proj_sum = jnp.zeros((TOKEN_POSITIONS, D), jnp.float32)
    for shard_index in range(N_TP):
        low_edge = shard_index * shard_width
        partial_value = jnp.dot(mixed[:, low_edge:low_edge + shard_width], out_weight[low_edge:low_edge + shard_width], preferred_element_type=jnp.float32)
        proj_sum = proj_sum + lax.optimization_barrier(partial_value.astype(jnp.bfloat16)).astype(jnp.float32)
    carried_rows = (hidden_in.astype(jnp.float32) + proj_sum).astype(jnp.bfloat16)
    normed = row_norm(carried_rows, mlp_gain)
    hidden_width = FF // N_TP
    mixer_sum = jnp.zeros((TOKEN_POSITIONS, D), jnp.float32)
    for shard_index in range(N_TP):
        low_edge = shard_index * hidden_width
        pre_act = jnp.dot(normed, up_weight[:, low_edge:low_edge + hidden_width], preferred_element_type=jnp.float32)
        squared = jnp.square(jax.nn.relu(pre_act)).astype(jnp.bfloat16)
        partial_value = lax.dot_general(squared, down_weight[:, low_edge:low_edge + hidden_width], (((1,), (1,)), ((), ())), preferred_element_type=jnp.float32)
        mixer_sum = mixer_sum + lax.optimization_barrier(partial_value.astype(jnp.bfloat16)).astype(jnp.float32)
    return (carried_rows.astype(jnp.float32) + mixer_sum).astype(jnp.bfloat16)
```

```python
import jax
import jax.numpy as jnp
from jax import lax
from jax.experimental import pallas as pl
from jax.experimental.pallas import tpu as pltpu
from jax.sharding import PartitionSpec as P

MESH = pl.DeviceIdType.MESH
BF, F32 = jnp.bfloat16, jnp.float32
EPS = 1e-06
NT = (((1,), (1,)), ((), ()))
STATES = 384
STEPS, LANES = 48, 8


def iota(shape, dim):
    return lax.broadcasted_iota(jnp.int32, shape, dim)


def one_row(values):
    rows, width = values.shape
    tiled = jnp.concatenate([values] * rows, axis=1)
    keep = iota(tiled.shape, 0) == iota(tiled.shape, 1) // width
    return jnp.sum(jnp.where(keep, tiled, 0.0), axis=0, keepdims=True)


def spread(column, width):
    rows = column.shape[0]
    shape = (rows, rows * width)
    keep = iota(shape, 0) == iota(shape, 1) // width
    return jnp.sum(jnp.where(keep, jnp.broadcast_to(column, shape), 0.0), axis=0, keepdims=True)


def expm1_small(x):
    total = jnp.ones_like(x)
    for order in range(9, 1, -1):
        total = 1.0 + total * x * (1.0 / order)
    return total * x


def times(a, b):
    return a[0] * b[0] - a[1] * b[1], a[0] * b[1] + a[1] * b[0]


def discretize(wide_poles, narrow_poles, log_step):
    real = jnp.concatenate([one_row(wide_poles[0]), one_row(narrow_poles[0])], axis=1)
    imag = jnp.concatenate([one_row(wide_poles[1]), one_row(narrow_poles[1])], axis=1)
    steps = log_step[...]
    step = jnp.exp(jnp.concatenate([spread(steps[:, :1], 64), spread(steps[:, 1:], 32)], axis=1))
    growth, angle = real * step, imag * step
    size, sine, cosine = jnp.exp(growth), jnp.sin(angle), jnp.cos(angle)
    half = jnp.sin(0.5 * angle)
    rise_real = expm1_small(growth) * cosine - 2.0 * half * half
    rise_imag = size * sine
    bottom = real * real + imag * imag
    coef_real = (rise_real * real + rise_imag * imag) / bottom
    coef_imag = (rise_imag * real - rise_real * imag) / bottom
    return (size * cosine, size * sine), (coef_real, coef_imag)


def in_blocks(wide_input, narrow_input):
    repeat = (iota((16, 128), 1) % 16 == iota((16, 128), 0)).astype(BF)
    out = []
    for part in range(2):
        for kind, (ref, width) in enumerate(((wide_input, 64), (narrow_input, 32))):
            flat = ref[part].reshape(4 * width, 16)
            tiled = jnp.dot(flat, repeat, preferred_element_type=F32)
            row, col = iota(tiled.shape, 0), iota(tiled.shape, 1)
            keep = (row // width == col // 32) & ((col // 16) % 2 == kind)
            out.append(jnp.where(keep, tiled, 0.0).astype(BF))
    return jnp.concatenate(out, axis=0)


def out_blocks(wide_output, narrow_output):
    out = []
    for part in range(2):
        halves = []
        for kind, (ref, width) in enumerate(((wide_output, 64), (narrow_output, 32))):
            flat = ref[part].reshape(64, width)
            row, col = iota((128, 64), 0), iota((128, 64), 1)
            pick = ((row // 32 == col // 16) & (row % 16 == col % 16)).astype(BF)
            rows = jnp.dot(pick, flat, preferred_element_type=F32).astype(BF)
            repeat = (iota((width, 4 * width), 1) % width == iota((width, 4 * width), 0)).astype(BF)
            tiled = jnp.dot(rows, repeat, preferred_element_type=F32)
            row, col = iota(tiled.shape, 0), iota(tiled.shape, 1)
            keep = (row // 32 == col // width) & ((row // 16) % 2 == kind)
            halves.append(jnp.where(keep, tiled, 0.0))
        whole = jnp.concatenate(halves, axis=1)
        out.append((whole if part == 0 else -whole).astype(BF))
    return out


def order():
    row, col = iota((384, 384), 0), iota((384, 384), 1)
    return (col == (row % LANES) * STEPS + row // LANES).astype(BF)


def back_order():
    row, col = iota((384, 384), 0), iota((384, 384), 1)
    return (row == (col % LANES) * STEPS + col // LANES).astype(BF)


def decay_rows(forget, pick):
    rows = jnp.concatenate([forget[p] for p in range(4)], axis=0)
    high = rows.astype(BF)
    rest = rows - high.astype(F32)
    middle = rest.astype(BF)
    low = (rest - middle.astype(F32)).astype(BF)
    parts = jnp.concatenate([high.astype(F32), middle.astype(F32), low.astype(F32)], axis=0).astype(BF)
    turned = lax.dot_general(pick, parts, NT, preferred_element_type=F32).astype(BF)
    row, col = iota((24, STATES), 0), iota((24, STATES), 1)
    group = jnp.where(col < 256, 2 * (col // 64), 2 * ((col - 256) // 32) + 1)
    place = (row % 8 == group).astype(BF)
    return jnp.exp(-jnp.dot(turned, place, preferred_element_type=F32))


def chain(first, ends, decay, run_base):
    now, starts = first, []
    for run in range(LANES):
        starts.append(now)
        part = slice(run, run + 1)
        grown = times(run_base, now)
        now = (
            decay[part] * grown[0] + ends[0][part],
            decay[part] * grown[1] + ends[1][part],
        )
    return [jnp.concatenate([s[i] for s in starts], axis=0) for i in range(2)], now


def kernel(
    hidden_in, drive, wide_poles, narrow_poles, log_step, forget, wide_input, narrow_input,
    wide_output, narrow_output, skip, mix_gain, out_weight, mlp_gain, up_weight, down_weight,
    out,
    up_a, up_b, dn_a, dn_b, mats, normed, part, final, own_in, carried, acc, pair_in, half_in, side_in,
    push_r, push_i, decay, ymsg, zmsg, gains, act_out, act_in, squared,
    loc_sem, s1_send, s1_recv, s2_send, s2_recv, y_send, y_recv, z_send, z_recv,
    g_send, g_recv, a_send, a_recv, ag_send, ag_recv, rs_send, rs_recv, out_sem,
):
    sp, tp = lax.axis_index("sp"), lax.axis_index("tp")
    y, z, x, core = sp % 8, sp // 8, tp // 2, tp % 2
    pending = []

    def along_y(step):
        return z * 8 + (y + step + 8) % 8, tp

    def along_z(step):
        return ((z + step + 8) % 8) * 8 + y, tp

    def group(step):
        return sp, (tp + step) % 8

    def along_x(step):
        return sp, ((x + step + 4) % 4) * 2 + core

    partner = (sp, 2 * x + 1 - core)

    def send(src, dst, send_sem, recv_sem, to):
        copy = pltpu.make_async_remote_copy(
            src_ref=src, dst_ref=dst, send_sem=send_sem, recv_sem=recv_sem, device_id=to, device_id_type=MESH
        )
        copy.start()
        pending.append(copy)

    def arrived(dst, recv_sem):
        pltpu.make_async_remote_copy(
            src_ref=dst, dst_ref=dst, send_sem=recv_sem, recv_sem=recv_sem, device_id=partner, device_id_type=MESH
        ).wait_recv()

    barrier = pltpu.get_barrier_semaphore()
    for step in range(1, 8):
        for to in (along_y(step), along_z(step), group(step)):
            pl.semaphore_signal(barrier, inc=1, device_id=to, device_id_type=MESH)
    bufs = (up_a, up_b, dn_a, dn_b)
    local = []
    for n, (weight, buf) in enumerate(zip((up_weight, up_weight, down_weight, down_weight), bufs)):
        local.append(
            pltpu.make_async_copy(weight.at[:, pl.ds((n % 2) * 512, 512)], buf.at[z, y], loc_sem.at[n])
        )
    local.append(pltpu.make_async_copy(out_weight, mats.at[tp], loc_sem.at[4]))
    local.append(pltpu.make_async_copy(hidden_in.at[pl.ds(pl.multiple_of(tp * 48, 16), 48)], own_in, loc_sem.at[5]))
    for copy in local:
        copy.start()
    for copy in local:
        copy.wait()
    pl.semaphore_wait(barrier, 21)

    def shard(n, first, second):
        return bufs[n].at[second, first] if n % 2 == 0 else bufs[n].at[first, second]

    def pair(n, q, second):
        both = pl.ds(2 * q, 2)
        return bufs[n].at[second, both] if n % 2 == 0 else bufs[n].at[both, second]

    def where_of(n):
        return (y, z, along_y, along_z) if n % 2 == 0 else (z, y, along_z, along_y)

    def mod8(v):
        return (v + 8) % 8

    def first_send(n, direction, hop):
        at, line, go, _ = where_of(n)
        k = (0 if direction > 0 else 4) + hop - 1
        ref = shard(n, mod8(at - direction * (hop - 1)), line)
        send(ref, ref, s1_send.at[n, k], s1_recv.at[n, k], go(direction))

    def first_wait(n, direction, hop):
        at, line, _, _ = where_of(n)
        k = (0 if direction > 0 else 4) + hop - 1
        arrived(shard(n, mod8(at - direction * hop), line), s1_recv.at[n, k])

    def first_start(n):
        first_send(n, 1, 1)
        first_send(n, -1, 1)

    def first_step(n, hop):
        first_wait(n, 1, hop)
        if hop < 4:
            first_send(n, 1, hop + 1)
            first_wait(n, -1, hop)
            if hop < 3:
                first_send(n, -1, hop + 1)

    def pair_at(n, r):
        at = where_of(n)[0]
        lean = 2 * (at % 2) - 1
        return (at // 2 + (0, lean, -lean, 2)[r] + 4) % 4

    def line_key(direction, hop, r):
        return (0 if direction > 0 else 16) + (hop - 1) * 4 + r

    def line_send(n, direction, hop, r):
        _, line, _, go = where_of(n)
        k = line_key(direction, hop, r)
        ref = pair(n, pair_at(n, r), mod8(line - direction * (hop - 1)))
        send(ref, ref, s2_send.at[n, k], s2_recv.at[n, k], go(direction))

    def line_wait(n, direction, hop, r):
        _, line, _, _ = where_of(n)
        k = line_key(direction, hop, r)
        arrived(pair(n, pair_at(n, r), mod8(line - direction * hop)), s2_recv.at[n, k])

    def line_start(ns, r):
        for n in ns:
            line_send(n, 1, 1, r)
            line_send(n, -1, 1, r)

    def line_step(ns, hop, r):
        for n in ns:
            for direction in (1, -1):
                last = r < 2 if direction > 0 else r >= 2
                if hop < 4 or last:
                    line_wait(n, direction, hop, r)
                    if hop < 3 or (hop == 3 and last):
                        line_send(n, direction, hop + 1, r)

    ups, downs = (0, 1), (2, 3)

    halves = (pl.ds(0, 1024), pl.ds(1024, 1024))

    def gather_start(buf, g):
        ref = buf.at[tp]
        send(ref, ref, ag_send.at[g, 0], ag_recv.at[g, 0], along_x(1))
        send(ref, ref, ag_send.at[g, 1], ag_recv.at[g, 1], along_x(-1))
        send(ref, ref, ag_send.at[g, 2], ag_recv.at[g, 2], partner)

    def gather_middle(buf, g):
        for n, direction in enumerate((1, -1)):
            ref = buf.at[along_x(-direction)[1]]
            arrived(ref, ag_recv.at[g, n])
            piece = ref.at[:, halves[n]]
            send(piece, piece, ag_send.at[g, 3 + n], ag_recv.at[g, 3 + n], along_x(direction))
            send(ref, ref, ag_send.at[g, 5 + n], ag_recv.at[g, 5 + n], partner)

    def gather_end(buf, g):
        far = buf.at[along_x(2)[1]]
        for n in range(2):
            piece = far.at[:, halves[n]]
            arrived(piece, ag_recv.at[g, 3 + n])
            send(piece, piece, ag_send.at[g, 7 + n], ag_recv.at[g, 7 + n], partner)

    def gather_partner(buf, g):
        def theirs(step):
            return buf.at[((x + step + 4) % 4) * 2 + 1 - core]

        arrived(theirs(0), ag_recv.at[g, 2])
        for n, direction in enumerate((1, -1)):
            arrived(theirs(-direction), ag_recv.at[g, 5 + n])
        for n in range(2):
            arrived(theirs(2).at[:, halves[n]], ag_recv.at[g, 7 + n])

    for n in range(4):
        first_start(n)
    gather_start(mats, 0)
    gains[tp] = mix_gain[...]
    for step in range(1, 8):
        send(mix_gain, gains.at[tp], g_send.at[step], g_recv.at[tp], group(step))

    pick = order()
    decay[...] = decay_rows(forget, pick)
    drive_now = jnp.dot(pick, drive[...], preferred_element_type=F32).astype(BF)
    for n in range(4):
        first_step(n, 1)
    line_start(ups, 0)
    base, coef = discretize(wide_poles, narrow_poles, log_step)
    pushed = lax.dot_general(drive_now, in_blocks(wide_input, narrow_input), NT, preferred_element_type=F32)
    pushed = times(coef, (pushed[:, :STATES], pushed[:, STATES:]))
    push_r[...] = pushed[0]
    push_i[...] = pushed[1]
    for n in range(4):
        first_step(n, 2)
    line_start(ups, 1)
    wide_base = [jnp.broadcast_to(b, (LANES, STATES)) for b in base]

    def scan_step(step, state):
        rows = pl.ds(pl.multiple_of(step * LANES, LANES), LANES)
        fade = decay[rows]
        grown = times(wide_base, state[:2])
        new = fade * grown[0] + push_r[rows], fade * grown[1] + push_i[rows], fade * state[2]
        push_r[rows], push_i[rows], decay[rows] = new
        return new

    zero = jnp.zeros((LANES, STATES), F32)
    end_r, end_i, total = lax.fori_loop(0, STEPS, scan_step, (zero, zero, zero + 1.0), unroll=4)
    powers = [base]
    for _ in range(5):
        powers.append(times(powers[-1], powers[-1]))
    run_base = times(powers[5], powers[4])
    _, last = chain((zero[:1], zero[:1]), (end_r, end_i), total, run_base)
    fade_all = total[:1]
    for run in range(1, LANES):
        fade_all = fade_all * total[run : run + 1]
    device_base = run_base
    for _ in range(3):
        device_base = times(device_base, device_base)
    line_base = device_base
    for _ in range(3):
        line_base = times(line_base, line_base)

    def message(buf, at, state, fade):
        buf[at] = jnp.concatenate([state[0], state[1], fade, jnp.zeros((5, STATES), F32)], axis=0)

    message(ymsg, y, last, fade_all)
    for step in range(1, 8):
        send(ymsg.at[y], ymsg.at[y], y_send.at[step], y_recv.at[y], along_y(step))
    for n in range(4):
        first_step(n, 3)
    line_start(ups, 2)
    for step in range(1, 8):
        arrived(ymsg.at[(y + step) % 8], y_recv.at[(y + step) % 8])
    zrow, onerow = zero[:1], zero[:1] + 1.0
    whole, before = (zrow, zrow), (zrow, zrow)
    whole_fade, before_fade, before_base = onerow, onerow, (onerow, zrow)
    for k in range(8):
        got = ymsg[k]
        fade = got[2:3]
        grown = times(device_base, whole)
        new = fade * grown[0] + got[0:1], fade * grown[1] + got[1:2]
        new_fade = whole_fade * fade
        new_base = times(before_base, device_base)
        earlier = k < y
        before = [jnp.where(earlier, n, o) for n, o in zip(new, before)]
        before_fade = jnp.where(earlier, new_fade, before_fade)
        before_base = [jnp.where(earlier, n, o) for n, o in zip(new_base, before_base)]
        whole, whole_fade = new, new_fade
    message(zmsg, z, whole, whole_fade)
    for step in range(1, 8):
        send(zmsg.at[z], zmsg.at[z], z_send.at[step], z_recv.at[z], along_z(step))
    for n in range(4):
        first_step(n, 4)
    line_start(ups, 3)
    for r in range(4):
        line_step(ups, 1, r)
    for step in range(1, 8):
        arrived(zmsg.at[(z + step) % 8], z_recv.at[(z + step) % 8])
    enter = (zrow, zrow)
    for k in range(8):
        got = zmsg[k]
        grown = times(line_base, enter)
        new = got[2:3] * grown[0] + got[0:1], got[2:3] * grown[1] + got[1:2]
        enter = [jnp.where(k < z, n, o) for n, o in zip(new, enter)]
    grown = times(before_base, enter)
    enter = before_fade * grown[0] + before[0], before_fade * grown[1] + before[1]
    starts, _ = chain(enter, (end_r, end_i), total, run_base)

    def fix_step(step, state):
        rows = pl.ds(pl.multiple_of(step * LANES, LANES), LANES)
        state = times(wide_base, state)
        push_r[rows] = push_r[rows] + decay[rows] * state[0]
        push_i[rows] = push_i[rows] + decay[rows] * state[1]
        return state

    lax.fori_loop(0, STEPS, fix_step, tuple(starts), unroll=4)
    real_block, imag_block = out_blocks(wide_output, narrow_output)
    response = lax.dot_general(push_r[...].astype(BF), real_block, NT, preferred_element_type=F32)
    response += lax.dot_general(push_i[...].astype(BF), imag_block, NT, preferred_element_type=F32)
    response += skip[...] * drive_now.astype(F32)
    active = 0.5 * response * (1.0 + lax.erf(response * (0.5**0.5)))
    active = jnp.dot(back_order(), active.astype(BF), preferred_element_type=F32).astype(BF)
    act_out[...] = active.reshape(8, 48, 128)
    act_in[tp] = act_out[tp]
    for step in range(1, 8):
        to = group(step)
        send(act_out.at[to[1]], act_in.at[tp], a_send.at[step], a_recv.at[tp], to)
    for r in range(4):
        line_step(ups, 2, r)
        line_start(downs, r)
    gather_middle(mats, 0)
    for step in range(1, 8):
        source = (tp + step) % 8
        arrived(gains.at[source], g_recv.at[source])
        arrived(act_in.at[source], a_recv.at[source])
    rows = jnp.concatenate([act_in[k] for k in range(8)], axis=1).astype(F32)
    gain = jnp.concatenate([gains[k] for k in range(8)], axis=1)
    power = jnp.sum(rows * rows, axis=1, keepdims=True) * (1.0 / 1024)
    mixed = (rows * lax.rsqrt(power + EPS) * gain).astype(BF)
    for r in range(4):
        line_step(ups, 3, r)
    gather_end(mats, 0)
    gather_partner(mats, 0)
    for n in range(8):
        cols = pl.ds(n * 256, 256)
        proj = jnp.dot(mixed, mats[:, :, cols].reshape(1024, 256), preferred_element_type=F32)
        carried[:, cols] = (own_in[:, cols].astype(F32) + proj).astype(BF)
    values = carried[...].astype(F32)
    power = jnp.sum(values * values, axis=1, keepdims=True) * (1.0 / 2048)
    normed[tp] = (values * lax.rsqrt(power + EPS) * mlp_gain[...]).astype(BF)
    gather_start(normed, 1)
    for r in range(4):
        line_step(ups, 4, r)
        line_step(downs, 1, r)
    gather_middle(normed, 1)
    for r in range(4):
        line_step(downs, 2, r)
    gather_end(normed, 1)
    gather_partner(normed, 1)

    for n in range(4):
        cols = pl.ds((n % 2) * 256, 256)
        pre = jnp.dot(
            normed[...].reshape(384, 2048),
            bufs[n // 2][:, :, :, cols].reshape(2048, 256),
            preferred_element_type=F32,
        )
        pre = jnp.maximum(pre, 0.0)
        squared[:, pl.ds(n * 256, 256)] = (pre * pre).astype(BF)
    for r in range(4):
        line_step(downs, 3, r)
    for r in range(4):
        line_step(downs, 4, r)
    for n in range(8):
        piece = lax.dot_general(squared[:, :512], dn_a[n].reshape(256, 512), NT, preferred_element_type=F32)
        piece += lax.dot_general(squared[:, 512:], dn_b[n].reshape(256, 512), NT, preferred_element_type=F32)
        part[:, :, :, pl.ds(n * 256, 256)] = piece.astype(BF).reshape(4, 2, 48, 256)

    def chip(step):
        return (x + step + 4) % 4

    for n, step in enumerate((2, 1, -1, 0)):
        to = chip(step)
        send(part.at[to, 1 - core], pair_in.at[to], rs_send.at[n], rs_recv.at[n], partner)

    def both(step, n):
        arrived(pair_in.at[chip(step)], rs_recv.at[n])
        return part[chip(step), core].astype(F32) + pair_in[chip(step)].astype(F32)

    acc[0] = both(2, 0).astype(BF)
    send(acc.at[0, :, halves[0]], half_in.at[0], rs_send.at[4], rs_recv.at[4], along_x(1))
    send(acc.at[0, :, halves[1]], half_in.at[1], rs_send.at[5], rs_recv.at[5], along_x(-1))
    right = both(1, 1)
    acc[1, :, 1024:] = right[:, 1024:].astype(BF)
    send(acc.at[1, :, halves[1]], side_in.at[0, :, halves[1]], rs_send.at[6], rs_recv.at[6], along_x(1))
    left = both(-1, 2)
    acc[2, :, :1024] = left[:, :1024].astype(BF)
    send(acc.at[2, :, halves[0]], side_in.at[1, :, halves[0]], rs_send.at[7], rs_recv.at[7], along_x(-1))
    arrived(half_in.at[0], rs_recv.at[4])
    acc[1, :, :1024] = (right[:, :1024] + half_in[0].astype(F32)).astype(BF)
    send(acc.at[1, :, halves[0]], side_in.at[0, :, halves[0]], rs_send.at[8], rs_recv.at[8], along_x(1))
    arrived(half_in.at[1], rs_recv.at[5])
    acc[2, :, 1024:] = (left[:, 1024:] + half_in[1].astype(F32)).astype(BF)
    send(acc.at[2, :, halves[1]], side_in.at[1, :, halves[1]], rs_send.at[9], rs_recv.at[9], along_x(-1))
    mine = both(0, 3) + carried[...].astype(F32)
    for copy in pending[:-13]:
        copy.wait_send()
    del pending[:-13]
    arrived(side_in.at[0, :, halves[1]], rs_recv.at[6])
    arrived(side_in.at[1, :, halves[0]], rs_recv.at[7])
    arrived(side_in.at[0, :, halves[0]], rs_recv.at[8])
    arrived(side_in.at[1, :, halves[1]], rs_recv.at[9])
    final[tp] = (mine + side_in[0].astype(F32) + side_in[1].astype(F32)).astype(BF)

    gather_start(final, 2)
    gather_middle(final, 2)
    gather_end(final, 2)
    gather_partner(final, 2)
    copy = pltpu.make_async_copy(final, out, out_sem)
    copy.start()
    for sent in pending:
        sent.wait_send()
    copy.wait()


def step(*args):
    args = list(args)
    for n in (10, 11, 13):
        args[n] = args[n].reshape(1, -1)
    vmem, hbm = pl.BlockSpec(memory_space=pltpu.VMEM), pl.BlockSpec(memory_space=pl.ANY)
    dma = pltpu.SemaphoreType.DMA
    scratch = [
        *[pltpu.VMEM((8, 8, 32, 512), BF)] * 4,
        pltpu.VMEM((8, 128, 2048), BF),
        pltpu.VMEM((8, 48, 2048), BF),
        pltpu.VMEM((4, 2, 48, 2048), BF),
        pltpu.VMEM((8, 48, 2048), BF),
        pltpu.VMEM((48, 2048), BF),
        pltpu.VMEM((48, 2048), BF),
        pltpu.VMEM((3, 48, 2048), BF),
        pltpu.VMEM((4, 48, 2048), BF),
        pltpu.VMEM((2, 48, 1024), BF),
        pltpu.VMEM((2, 48, 2048), BF),
        *[pltpu.VMEM((384, STATES), F32)] * 3,
        *[pltpu.VMEM((8, 8, STATES), F32)] * 2,
        pltpu.VMEM((8, 1, 128), F32),
        pltpu.VMEM((8, 48, 128), BF),
        pltpu.VMEM((8, 48, 128), BF),
        pltpu.VMEM((384, 1024), BF),
        dma((6,)), dma((4, 7)), dma((4, 7)), dma((4, 32)), dma((4, 32)),
        *[dma((8,))] * 8,
        dma((3, 9)), dma((3, 9)), dma((10,)), dma((10,)), dma,
    ]
    whole = pl.pallas_call(
        kernel,
        out_shape=jax.ShapeDtypeStruct((8, 48, 2048), BF),
        in_specs=[hbm if n in (0, 12, 14, 15) else vmem for n in range(16)],
        out_specs=hbm,
        scratch_shapes=scratch,
        compiler_params=pltpu.CompilerParams(
            collective_id=0, has_side_effects=True, vmem_limit_bytes=60 * 1024 * 1024
        ),
    )(*args)
    return whole.reshape(384, 2048)


def solution(mesh):
    return jax.shard_map(
        step,
        mesh=mesh,
        in_specs=(
            P("sp", None),
            P("sp", "tp"),
            P(None, "tp", None),
            P(None, "tp", None),
            P("tp", None),
            P("tp", None, "sp"),
            P(None, "tp", None, None),
            P(None, "tp", None, None),
            P(None, "tp", None, None),
            P(None, "tp", None, None),
            P("tp"),
            P("tp"),
            P("tp", None),
            P(),
            P("sp", "tp"),
            P("sp", "tp"),
        ),
        out_specs=P("sp", None),
        check_vma=False,
    )
```

```python
import jax
import jax.numpy as jnp
from jax import lax
from jax.experimental import pallas as pl
from jax.experimental.pallas import tpu as pltpu
from jax.sharding import PartitionSpec as P

MESH = pl.DeviceIdType.MESH
BF, F32 = jnp.bfloat16, jnp.float32
EPS = 1e-06
NT = (((1,), (1,)), ((), ()))
STATES = 384
STEPS, LANES = 48, 8


def iota(shape, dim):
    return lax.broadcasted_iota(jnp.int32, shape, dim)


def one_row(values):
    rows, width = values.shape
    tiled = jnp.concatenate([values] * rows, axis=1)
    keep = iota(tiled.shape, 0) == iota(tiled.shape, 1) // width
    return jnp.sum(jnp.where(keep, tiled, 0.0), axis=0, keepdims=True)


def spread(line, width):
    keep = iota((4, 4), 0) == iota((4, 4), 1)
    column = jnp.sum(jnp.where(keep, jnp.broadcast_to(line, (4, 4)), 0.0), axis=1, keepdims=True)
    shape = (4, 4 * width)
    keep = iota(shape, 0) == iota(shape, 1) // width
    return jnp.sum(jnp.where(keep, jnp.broadcast_to(column, shape), 0.0), axis=0, keepdims=True)


def expm1_small(x):
    total = jnp.ones_like(x)
    for order in range(9, 1, -1):
        total = 1.0 + total * x * (1.0 / order)
    return total * x


def times(a, b):
    return a[0] * b[0] - a[1] * b[1], a[0] * b[1] + a[1] * b[0]


def discretize(wide_poles, narrow_poles, log_step):
    real = jnp.concatenate([one_row(wide_poles[0]), one_row(narrow_poles[0])], axis=1)
    imag = jnp.concatenate([one_row(wide_poles[1]), one_row(narrow_poles[1])], axis=1)
    steps = log_step[...]
    step = jnp.exp(jnp.concatenate([spread(steps[:1], 64), spread(steps[1:], 32)], axis=1))
    growth, angle = real * step, imag * step
    size, sine, cosine = jnp.exp(growth), jnp.sin(angle), jnp.cos(angle)
    half = jnp.sin(0.5 * angle)
    rise_real = expm1_small(growth) * cosine - 2.0 * half * half
    rise_imag = size * sine
    bottom = real * real + imag * imag
    coef_real = (rise_real * real + rise_imag * imag) / bottom
    coef_imag = (rise_imag * real - rise_real * imag) / bottom
    return (size * cosine, size * sine), (coef_real, coef_imag)


def blocks(first, second):
    out = []
    for part in range(2):
        halves = []
        for kind, (ref, width) in enumerate(((first, 64), (second, 32))):
            flat = ref[part].reshape(64, width)
            row, col = iota((128, 64), 0), iota((128, 64), 1)
            pick = ((row // 32 == col // 16) & (row % 16 == col % 16)).astype(BF)
            rows = jnp.dot(pick, flat, preferred_element_type=F32).astype(BF)
            repeat = (iota((width, 4 * width), 1) % width == iota((width, 4 * width), 0)).astype(BF)
            tiled = jnp.dot(rows, repeat, preferred_element_type=F32)
            row, col = iota(tiled.shape, 0), iota(tiled.shape, 1)
            keep = (row // 32 == col // width) & ((row // 16) % 2 == kind)
            halves.append(jnp.where(keep, tiled, 0.0))
        out.append(jnp.concatenate(halves, axis=1))
    return out


def order():
    row, col = iota((384, 384), 0), iota((384, 384), 1)
    return (col == (row % LANES) * STEPS + row // LANES).astype(BF)


def back_order():
    row, col = iota((384, 384), 0), iota((384, 384), 1)
    return (row == (col % LANES) * STEPS + col // LANES).astype(BF)


def decay_rows(forget, pick):
    rows = jnp.concatenate([forget[p] for p in range(4)], axis=0)
    high = rows.astype(BF)
    rest = rows - high.astype(F32)
    middle = rest.astype(BF)
    low = (rest - middle.astype(F32)).astype(BF)
    parts = jnp.concatenate([high.astype(F32), middle.astype(F32), low.astype(F32)], axis=0).astype(BF)
    turned = lax.dot_general(pick, parts, NT, preferred_element_type=F32).astype(BF)
    row, col = iota((24, STATES), 0), iota((24, STATES), 1)
    group = jnp.where(col < 256, 2 * (col // 64), 2 * ((col - 256) // 32) + 1)
    place = (row % 8 == group).astype(BF)
    return jnp.exp(-jnp.dot(turned, place, preferred_element_type=F32))


def chain(first, ends, decay, run_base):
    now, starts = first, []
    for run in range(LANES):
        starts.append(now)
        part = slice(run, run + 1)
        grown = times(run_base, now)
        now = (
            decay[part] * grown[0] + ends[0][part],
            decay[part] * grown[1] + ends[1][part],
        )
    return [jnp.concatenate([s[i] for s in starts], axis=0) for i in range(2)], now


def kernel(
    hidden_in, drive, wide_poles, narrow_poles, log_step, forget, wide_input, narrow_input,
    wide_output, narrow_output, skip, mix_gain, out_weight, mlp_gain, up_weight, down_weight,
    out,
    up_a, up_b, dn_a, dn_b, mats, normed, part, own_in, carried, acc, pair_in, half_in, side_in,
    push_r, push_i, decay, ymsg, zmsg, gains, act_out, act_in, squared,
    loc_sem, w_send, s1_recv, s2_recv, m_send, m_recv, ag_send, ag_recv, t_send, t_recv,
):
    sp, tp = lax.axis_index("sp"), lax.axis_index("tp")
    y, z, x, core = sp % 8, sp // 8, tp // 2, tp % 2

    def along_y(step):
        return z * 8 + (y + step + 8) % 8, tp

    def along_z(step):
        return ((z + step + 8) % 8) * 8 + y, tp

    def group(step):
        return sp, (tp + step) % 8

    def along_x(step):
        return sp, ((x + step + 4) % 4) * 2 + core

    partner = (sp, 2 * x + 1 - core)

    def send(src, dst, send_sem, recv_sem, to):
        pltpu.make_async_remote_copy(
            src_ref=src, dst_ref=dst, send_sem=send_sem, recv_sem=recv_sem, device_id=to, device_id_type=MESH
        ).start()

    def held(ref, sem):
        return pltpu.make_async_remote_copy(
            src_ref=ref, dst_ref=ref, send_sem=sem, recv_sem=sem, device_id=partner, device_id_type=MESH
        )

    def arrived(dst, recv_sem):
        held(dst, recv_sem).wait_recv()

    def left(src, send_sem):
        held(src, send_sem).wait_send()

    barrier = pltpu.get_barrier_semaphore()
    for step in range(1, 8):
        for to in (along_y(step), along_z(step), group(step)):
            pl.semaphore_signal(barrier, inc=1, device_id=to, device_id_type=MESH)
    bufs = (up_a, up_b, dn_a, dn_b)

    def where_of(n):
        return (y, z, along_y, along_z) if n % 2 == 0 else (z, y, along_z, along_y)

    def shard(n, first, second):
        return bufs[n].at[second * 8 + first]

    def pair(n, q, second):
        return bufs[n].at[pl.ds(second * 8 + 2 * q, 2)]

    def mod8(v):
        return (v + 8) % 8

    local = []
    for n, weight in enumerate((up_weight, up_weight, down_weight, down_weight)):
        at, line, _, _ = where_of(n)
        local.append(
            pltpu.make_async_copy(weight.at[:, pl.ds((n % 2) * 512, 512)], shard(n, at, line), loc_sem.at[n])
        )
    local.append(pltpu.make_async_copy(out_weight, mats.at[tp], loc_sem.at[4]))
    local.append(pltpu.make_async_copy(hidden_in.at[pl.ds(pl.multiple_of(tp * 48, 16), 48)], own_in, loc_sem.at[5]))
    for copy in local:
        copy.start()
    def first_key(direction, hop):
        return (0 if direction > 0 else 4) + hop - 1

    def direct_start(n):
        at, line, go, _ = where_of(n)
        ref = shard(n, at, line)
        for hop in range(1, 5):
            for direction in (1, -1) if hop < 4 else (1,):
                send(ref, ref, w_send.at[n], s1_recv.at[n, first_key(direction, hop)], go(direction * hop))

    def first_send(n, direction, hop):
        at, line, go, _ = where_of(n)
        ref = shard(n, mod8(at - direction * (hop - 1)), line)
        send(ref, ref, w_send.at[n], s1_recv.at[n, first_key(direction, hop)], go(direction))

    def first_wait(n, direction, hop):
        at, line, _, _ = where_of(n)
        arrived(shard(n, mod8(at - direction * hop), line), s1_recv.at[n, first_key(direction, hop)])

    def direct_wait(n, hop):
        first_wait(n, 1, hop)
        if hop < 4:
            first_wait(n, -1, hop)

    def first_step(n, hop):
        first_wait(n, 1, hop)
        if hop < 4:
            first_send(n, 1, hop + 1)
            first_wait(n, -1, hop)
            if hop < 3:
                first_send(n, -1, hop + 1)

    def pair_at(n, r):
        at = where_of(n)[0]
        lean = 2 * (at % 2) - 1
        return (at // 2 + (0, lean, -lean, 2)[r] + 4) % 4

    def line_key(direction, hop, r):
        if hop == 4:
            return 24 + r
        return (0 if direction > 0 else 12) + (hop - 1) * 4 + r

    def line_send(n, direction, hop, r):
        _, line, _, go = where_of(n)
        ref = pair(n, pair_at(n, r), mod8(line - direction * (hop - 1)))
        send(ref, ref, w_send.at[n], s2_recv.at[n, line_key(direction, hop, r)], go(direction))

    def line_wait(n, direction, hop, r):
        _, line, _, _ = where_of(n)
        arrived(pair(n, pair_at(n, r), mod8(line - direction * hop)), s2_recv.at[n, line_key(direction, hop, r)])

    def line_start(ns, r):
        for n in ns:
            line_send(n, 1, 1, r)
            line_send(n, -1, 1, r)

    def line_step(ns, hop, r):
        for n in ns:
            for direction in (1, -1):
                last = r < 2 if direction > 0 else r >= 2
                if hop < 4 or last:
                    line_wait(n, direction, hop, r)
                    if hop < 3 or (hop == 3 and last):
                        line_send(n, direction, hop + 1, r)

    ups, downs = (0, 1), (2, 3)

    halves = (pl.ds(0, 1024), pl.ds(1024, 1024))

    def gather_start(buf, g):
        ref = buf.at[tp]
        for turn in range(2):
            for n, direction in enumerate((1, -1)):
                half = (n + turn) % 2
                piece = ref.at[:, halves[half]]
                send(piece, piece, ag_send.at[g], ag_recv.at[g, 2 * n + turn], along_x(direction))
        send(ref, ref, ag_send.at[g], ag_recv.at[g, 6], partner)

    def gather_middle(buf, g, turns=(0, 1)):
        for turn in turns:
            for n, direction in enumerate((1, -1)):
                half = (n + turn) % 2
                piece = buf.at[along_x(-direction)[1], :, halves[half]]
                arrived(piece, ag_recv.at[g, 2 * n + turn])
                if turn == 0:
                    send(piece, piece, ag_send.at[g], ag_recv.at[g, 4 + n], along_x(direction))
                send(piece, piece, ag_send.at[g], ag_recv.at[g, 6], partner)

    def gather_end(buf, g):
        far = buf.at[along_x(2)[1]]
        for n in range(2):
            piece = far.at[:, halves[n]]
            arrived(piece, ag_recv.at[g, 4 + n])
            send(piece, piece, ag_send.at[g], ag_recv.at[g, 6], partner)

    def gather_partner(buf, g):
        arrived(buf.at[pl.ds(0, 4)], ag_recv.at[g, 6])

    def message(buf, at, state, fade):
        buf[at] = jnp.concatenate([state[0], state[1], fade, fade], axis=0)

    pick = order()
    decay[...] = decay_rows(forget, pick)
    drive_now = jnp.dot(pick, drive[...], preferred_element_type=F32).astype(BF)
    base, coef = discretize(wide_poles, narrow_poles, log_step)
    weights = [b.astype(BF) for b in blocks(wide_input, narrow_input)]
    pushed = times(coef, [jnp.dot(drive_now, w, preferred_element_type=F32) for w in weights])
    push_r[...] = pushed[0]
    push_i[...] = pushed[1]
    wide_base = [jnp.broadcast_to(b, (LANES, STATES)) for b in base]

    def scan_step(step, state):
        rows = pl.ds(pl.multiple_of(step * LANES, LANES), LANES)
        fade = decay[rows]
        grown = times(wide_base, state[:2])
        new = fade * grown[0] + push_r[rows], fade * grown[1] + push_i[rows], fade * state[2]
        push_r[rows], push_i[rows], decay[rows] = new
        return new

    zero = jnp.zeros((LANES, STATES), F32)
    end_r, end_i, total = lax.fori_loop(0, STEPS, scan_step, (zero, zero, zero + 1.0), unroll=4)
    powers = [base]
    for _ in range(5):
        powers.append(times(powers[-1], powers[-1]))
    run_base = times(powers[5], powers[4])
    _, last = chain((zero[:1], zero[:1]), (end_r, end_i), total, run_base)
    fade_all = total[:1]
    for run in range(1, LANES):
        fade_all = fade_all * total[run : run + 1]
    device_base = run_base
    for _ in range(3):
        device_base = times(device_base, device_base)
    line_base = device_base
    for _ in range(3):
        line_base = times(line_base, line_base)

    for copy in local:
        copy.wait()
    pl.semaphore_wait(barrier, 21)

    message(ymsg, y, last, fade_all)
    for step in range(1, 8):
        send(ymsg.at[y], ymsg.at[y], m_send.at[1], m_recv.at[1], along_y(step))
    for n in range(4):
        first_send(n, 1, 1)
        first_send(n, -1, 1)
    gather_start(mats, 0)
    gains[tp] = mix_gain[...]
    for step in range(1, 8):
        send(mix_gain, gains.at[tp], m_send.at[0], m_recv.at[0], group(step))
    for n in range(4):
        first_step(n, 1)
    line_start(ups, 0)
    arrived(ymsg.at[pl.ds(0, 7)], m_recv.at[1])
    zrow, onerow = zero[:1], zero[:1] + 1.0
    whole, before = (zrow, zrow), (zrow, zrow)
    whole_fade, before_fade, before_base = onerow, onerow, (onerow, zrow)
    for k in range(8):
        got = ymsg[k]
        fade = got[2:3]
        grown = times(device_base, whole)
        new = fade * grown[0] + got[0:1], fade * grown[1] + got[1:2]
        new_fade = whole_fade * fade
        new_base = times(before_base, device_base)
        earlier = k < y
        before = [jnp.where(earlier, n, o) for n, o in zip(new, before)]
        before_fade = jnp.where(earlier, new_fade, before_fade)
        before_base = [jnp.where(earlier, n, o) for n, o in zip(new_base, before_base)]
        whole, whole_fade = new, new_fade
    message(zmsg, z, whole, whole_fade)
    for step in range(1, 8):
        send(zmsg.at[z], zmsg.at[z], m_send.at[2], m_recv.at[2], along_z(step))
    for n in range(4):
        first_step(n, 2)
    line_start(ups, 1)
    line_step(ups, 1, 0)
    for n in range(4):
        first_step(n, 3)
    line_start(ups, 2)
    arrived(zmsg.at[pl.ds(0, 7)], m_recv.at[2])
    enter = (zrow, zrow)
    for k in range(8):
        got = zmsg[k]
        grown = times(line_base, enter)
        new = got[2:3] * grown[0] + got[0:1], got[2:3] * grown[1] + got[1:2]
        enter = [jnp.where(k < z, n, o) for n, o in zip(new, enter)]
    grown = times(before_base, enter)
    enter = before_fade * grown[0] + before[0], before_fade * grown[1] + before[1]
    line_step(ups, 1, 1)
    for n in range(4):
        first_step(n, 4)
    line_start(ups, 3)
    starts, _ = chain(enter, (end_r, end_i), total, run_base)

    def fix_step(step, state):
        rows = pl.ds(pl.multiple_of(step * LANES, LANES), LANES)
        state = times(wide_base, state)
        push_r[rows] = push_r[rows] + decay[rows] * state[0]
        push_i[rows] = push_i[rows] + decay[rows] * state[1]
        return state

    lax.fori_loop(0, STEPS, fix_step, tuple(starts), unroll=4)
    real_block, imag_block = blocks(wide_output, narrow_output)
    response = lax.dot_general(push_r[...].astype(BF), real_block.astype(BF), NT, preferred_element_type=F32)
    response -= lax.dot_general(push_i[...].astype(BF), imag_block.astype(BF), NT, preferred_element_type=F32)
    response += skip[...] * drive_now.astype(F32)
    active = 0.5 * response * (1.0 + lax.erf(response * (0.5**0.5)))
    active = jnp.dot(back_order(), active.astype(BF), preferred_element_type=F32).astype(BF)
    act_out[...] = active.reshape(8, 48, 128)
    act_in[tp] = act_out[tp]
    for step in range(1, 8):
        to = group(step)
        send(act_out.at[to[1]], act_in.at[tp], m_send.at[3], m_recv.at[3], to)
    line_step(ups, 2, 0)
    line_step(ups, 1, 2)
    line_step(ups, 2, 1)
    line_step(ups, 1, 3)
    gather_middle(mats, 0, (0,))
    line_start(downs, 0)
    line_step(ups, 2, 2)
    line_start(downs, 1)
    arrived(gains.at[pl.ds(0, 7)], m_recv.at[0])
    arrived(act_in.at[pl.ds(0, 7)], m_recv.at[3])
    rows = jnp.concatenate([act_in[k] for k in range(8)], axis=1).astype(F32)
    gain = jnp.concatenate([gains[k] for k in range(8)], axis=1)
    power = jnp.sum(rows * rows, axis=1, keepdims=True) * (1.0 / 1024)
    mixed = (rows * lax.rsqrt(power + EPS) * gain).astype(BF)
    line_step(ups, 2, 3)
    gather_middle(mats, 0, (1,))
    line_step(ups, 3, 0)
    line_start((2,), 2)
    line_step(ups, 3, 1)
    line_start((2,), 3)
    gather_end(mats, 0)
    gather_partner(mats, 0)
    for n in range(8):
        cols = pl.ds(n * 256, 256)
        proj = jnp.dot(mixed, mats[:, :, cols].reshape(1024, 256), preferred_element_type=F32)
        carried[:, cols] = (own_in[:, cols].astype(F32) + proj).astype(BF)
    values = carried[...].astype(F32)
    power = jnp.sum(values * values, axis=1, keepdims=True) * (1.0 / 2048)
    normed[tp] = (values * lax.rsqrt(power + EPS) * mlp_gain[...]).astype(BF)
    gather_start(normed, 1)
    def down_at(pos):
        line_step((2,), pos // 4 + 1, pos % 4)
        line_step((3,), pos % 8 // 2 + 1, pos % 2 + 2 * (pos // 8))

    line_step(ups, 3, 2)
    line_step(ups, 3, 3)
    down_at(0)
    line_step(ups, 4, 0)
    line_step(ups, 4, 1)
    gather_middle(normed, 1, (0,))
    line_step(ups, 4, 2)
    line_step(ups, 4, 3)
    down_at(1)
    gather_middle(normed, 1, (1,))
    down_at(2)
    gather_end(normed, 1)
    down_at(3)
    gather_partner(normed, 1)

    for n in range(4):
        cols = pl.ds((n % 2) * 256, 256)
        buf = bufs[n // 2]
        if n < 2:
            weight = buf[:, :, cols].reshape(2048, 256)
        else:
            weight = jnp.concatenate([buf[(s % 8) * 8 + s // 8, :, cols] for s in range(64)], axis=0)
        pre = jnp.dot(normed[...].reshape(384, 2048), weight, preferred_element_type=F32)
        pre = jnp.maximum(pre, 0.0)
        squared[:, pl.ds(n * 256, 256)] = (pre * pre).astype(BF)

    def chip(step):
        return (x + step + 4) % 4

    small = (pl.ds(0, 256), pl.ds(256, 256))

    def columns(r, half=None):
        start = pair_at(3, r) * 512
        if half is None:
            return pl.ds(pl.multiple_of(start, 512), 512)
        return pl.ds(pl.multiple_of(start + half * 256, 256), 256)

    def product(r):
        q = pair_at(3, r)
        first = dn_a[pl.ds(pl.multiple_of(q * 16, 16), 16)].reshape(512, 512)
        second = jnp.concatenate([dn_b[(s % 8) * 8 + 2 * q + s // 8] for s in range(16)], axis=0)
        piece = lax.dot_general(squared[:, :512], first, NT, preferred_element_type=F32)
        piece += lax.dot_general(squared[:, 512:], second, NT, preferred_element_type=F32)
        piece = piece.astype(BF)
        for b in range(8):
            part[r * 8 + (b % 2) * 4 + b // 2] = piece[b * 48 : (b + 1) * 48]
        send(part.at[pl.ds(r * 8 + (1 - core) * 4, 4)], pair_in.at[r], t_send.at[r], t_recv.at[r, 0], partner)

    def chip_sum(r, step):
        return part[r * 8 + core * 4 + chip(step)].astype(F32) + pair_in[r, chip(step)].astype(F32)

    def sums_out(r):
        arrived(pair_in.at[r], t_recv.at[r, 0])
        acc[r, 0] = chip_sum(r, 2).astype(BF)
        for n, direction in enumerate((1, -1)):
            send(acc.at[r, 0, :, small[n]], half_in.at[r, n], t_send.at[r], t_recv.at[r, 1 + n], along_x(direction))
        for n, direction in enumerate((1, -1)):
            acc[r, 1 + n] = chip_sum(r, direction).astype(BF)
            ready = small[1 - n]
            send(
                acc.at[r, 1 + n, :, ready], side_in.at[r, n, :, ready],
                t_send.at[r], t_recv.at[r, 3], along_x(direction),
            )

    def sums_on(r):
        for n, direction in enumerate((1, -1)):
            arrived(half_in.at[r, n], t_recv.at[r, 1 + n])
            cols = slice(n * 256, (n + 1) * 256)
            acc[r, 1 + n, :, cols] = (chip_sum(r, direction)[:, cols] + half_in[r, n].astype(F32)).astype(BF)
            send(
                acc.at[r, 1 + n, :, small[n]], side_in.at[r, n, :, small[n]],
                t_send.at[r], t_recv.at[r, 3], along_x(direction),
            )

    def finish(r):
        mine = chip_sum(r, 0) + carried[:, columns(r)].astype(F32)
        arrived(side_in.at[r], t_recv.at[r, 3])
        out[tp, :, columns(r)] = (mine + side_in[r, 0].astype(F32) + side_in[r, 1].astype(F32)).astype(BF)
        ref = out.at[tp, :, columns(r)]
        for n, direction in enumerate((1, -1)):
            send(ref, ref, t_send.at[r], t_recv.at[r, 4 + n], along_x(direction))
        send(ref, ref, t_send.at[r], t_recv.at[r, 8], partner)

    def pass_on(r):
        for n, direction in enumerate((1, -1)):
            at = along_x(-direction)[1]
            arrived(out.at[at, :, columns(r)], t_recv.at[r, 4 + n])
            piece = out.at[at, :, columns(r, n)]
            send(piece, piece, t_send.at[r], t_recv.at[r, 6 + n], along_x(direction))
            ref = out.at[at, :, columns(r)]
            send(ref, ref, t_send.at[r], t_recv.at[r, 8], partner)

    def pass_last(r):
        for n in range(2):
            piece = out.at[along_x(2)[1], :, columns(r, n)]
            arrived(piece, t_recv.at[r, 6 + n])
            send(piece, piece, t_send.at[r], t_recv.at[r, 8], partner)

    for pos in range(4, 7):
        down_at(pos)
    line_start((3,), 2)
    line_start((3,), 3)
    product(0)
    down_at(7)
    product(1)
    sums_out(0)
    down_at(8)
    sums_out(1)
    down_at(9)
    sums_on(0)
    down_at(10)
    sums_on(1)
    finish(0)
    down_at(11)
    finish(1)
    down_at(12)
    pass_on(0)
    down_at(13)
    pass_on(1)
    down_at(14)
    pass_last(0)
    down_at(15)
    product(2)
    product(3)
    pass_last(1)
    for n in range(4):
        left(bufs[n].at[pl.ds(0, 63)], w_send.at[n])
    left(gains.at[pl.ds(0, 7)], m_send.at[0])
    left(ymsg.at[pl.ds(0, 7)], m_send.at[1])
    left(zmsg.at[pl.ds(0, 7)], m_send.at[2])
    left(act_out.at[pl.ds(0, 7)], m_send.at[3])
    left(mats.at[pl.ds(0, 7)], ag_send.at[0])
    left(normed.at[pl.ds(0, 7)], ag_send.at[1])
    for r in (2, 3):
        sums_out(r)
    for r in (2, 3):
        sums_on(r)
    for r in (2, 3):
        finish(r)
    for r in (2, 3):
        pass_on(r)
    for r in (2, 3):
        pass_last(r)
    for r in range(4):
        arrived(part.at[pl.ds(0, 4)], t_recv.at[r, 8])
    for r in range(4):
        left(part.at[pl.ds(0, 14)], t_send.at[r])


def step(*args):
    args = list(args)
    for n in (10, 11, 13):
        args[n] = args[n].reshape(1, -1)
    args[4] = args[4].T
    for n in (6, 7):
        args[n] = jnp.swapaxes(args[n], 2, 3)
    vmem, hbm = pl.BlockSpec(memory_space=pltpu.VMEM), pl.BlockSpec(memory_space=pltpu.HBM)
    dma = pltpu.SemaphoreType.DMA
    scratch = [
        *[pltpu.VMEM((64, 32, 512), BF)] * 4,
        pltpu.VMEM((8, 128, 2048), BF),
        pltpu.VMEM((8, 48, 2048), BF),
        pltpu.VMEM((32, 48, 512), BF),
        pltpu.VMEM((48, 2048), BF),
        pltpu.VMEM((48, 2048), BF),
        pltpu.VMEM((4, 3, 48, 512), BF),
        pltpu.VMEM((4, 4, 48, 512), BF),
        pltpu.VMEM((4, 2, 48, 256), BF),
        pltpu.VMEM((4, 2, 48, 512), BF),
        *[pltpu.VMEM((384, STATES), F32)] * 3,
        *[pltpu.VMEM((8, 4, STATES), F32)] * 2,
        pltpu.VMEM((8, 1, 128), F32),
        pltpu.VMEM((8, 48, 128), BF),
        pltpu.VMEM((8, 48, 128), BF),
        pltpu.VMEM((384, 1024), BF),
        dma((6,)), dma((4,)), dma((4, 7)), dma((4, 28)), dma((4,)), dma((4,)),
        dma((2,)), dma((2, 7)), dma((4,)), dma((4, 9)),
    ]
    whole = pl.pallas_call(
        kernel,
        out_shape=jax.ShapeDtypeStruct((8, 48, 2048), BF),
        in_specs=[hbm if n in (0, 12, 14, 15) else vmem for n in range(16)],
        out_specs=vmem,
        scratch_shapes=scratch,
        compiler_params=pltpu.CompilerParams(
            collective_id=0, has_side_effects=True, vmem_limit_bytes=58 * 1024 * 1024
        ),
    )(*args)
    return whole.reshape(384, 2048)


def solution(mesh):
    return jax.shard_map(
        step,
        mesh=mesh,
        in_specs=(
            P("sp", None),
            P("sp", "tp"),
            P(None, "tp", None),
            P(None, "tp", None),
            P("tp", None),
            P("tp", None, "sp"),
            P(None, "tp", None, None),
            P(None, "tp", None, None),
            P(None, "tp", None, None),
            P(None, "tp", None, None),
            P("tp"),
            P("tp"),
            P("tp", None),
            P(),
            P("sp", "tp"),
            P("sp", "tp"),
        ),
        out_specs=P("sp", None),
        check_vma=False,
    )
```

```python
import jax
import jax.numpy as jnp
from jax import lax
from jax.experimental import pallas as pl
from jax.experimental.pallas import tpu as pltpu
from jax.sharding import PartitionSpec as P

MESH = pl.DeviceIdType.MESH
BF, F32 = jnp.bfloat16, jnp.float32
EPS = 1e-06
NT = (((1,), (1,)), ((), ()))
STATES = 384
STEPS, LANES = 48, 8


def iota(shape, dim):
    return lax.broadcasted_iota(jnp.int32, shape, dim)


def one_row(values):
    rows, width = values.shape
    tiled = jnp.concatenate([values] * rows, axis=1)
    keep = iota(tiled.shape, 0) == iota(tiled.shape, 1) // width
    return jnp.sum(jnp.where(keep, tiled, 0.0), axis=0, keepdims=True)


def spread(line, width):
    keep = iota((4, 4), 0) == iota((4, 4), 1)
    column = jnp.sum(jnp.where(keep, jnp.broadcast_to(line, (4, 4)), 0.0), axis=1, keepdims=True)
    shape = (4, 4 * width)
    keep = iota(shape, 0) == iota(shape, 1) // width
    return jnp.sum(jnp.where(keep, jnp.broadcast_to(column, shape), 0.0), axis=0, keepdims=True)


def expm1_small(x):
    total = jnp.ones_like(x)
    for order in range(9, 1, -1):
        total = 1.0 + total * x * (1.0 / order)
    return total * x


def times(a, b):
    return a[0] * b[0] - a[1] * b[1], a[0] * b[1] + a[1] * b[0]


def discretize(wide_poles, narrow_poles, log_step):
    real = jnp.concatenate([one_row(wide_poles[0]), one_row(narrow_poles[0])], axis=1)
    imag = jnp.concatenate([one_row(wide_poles[1]), one_row(narrow_poles[1])], axis=1)
    steps = log_step[...]
    step = jnp.exp(jnp.concatenate([spread(steps[:1], 64), spread(steps[1:], 32)], axis=1))
    growth, angle = real * step, imag * step
    size, sine, cosine = jnp.exp(growth), jnp.sin(angle), jnp.cos(angle)
    half = jnp.sin(0.5 * angle)
    rise_real = expm1_small(growth) * cosine - 2.0 * half * half
    rise_imag = size * sine
    bottom = real * real + imag * imag
    coef_real = (rise_real * real + rise_imag * imag) / bottom
    coef_imag = (rise_imag * real - rise_real * imag) / bottom
    return (size * cosine, size * sine), (coef_real, coef_imag)


def blocks(first, second):
    out = []
    for part in range(2):
        halves = []
        for kind, (ref, width) in enumerate(((first, 64), (second, 32))):
            flat = ref[part].reshape(64, width)
            row, col = iota((128, 64), 0), iota((128, 64), 1)
            pick = ((row // 32 == col // 16) & (row % 16 == col % 16)).astype(BF)
            rows = jnp.dot(pick, flat, preferred_element_type=F32).astype(BF)
            repeat = (iota((width, 4 * width), 1) % width == iota((width, 4 * width), 0)).astype(BF)
            tiled = jnp.dot(rows, repeat, preferred_element_type=F32)
            row, col = iota(tiled.shape, 0), iota(tiled.shape, 1)
            keep = (row // 32 == col // width) & ((row // 16) % 2 == kind)
            halves.append(jnp.where(keep, tiled, 0.0))
        out.append(jnp.concatenate(halves, axis=1))
    return out


def order():
    row, col = iota((384, 384), 0), iota((384, 384), 1)
    return (col == (row % LANES) * STEPS + row // LANES).astype(BF)


def back_order():
    row, col = iota((384, 384), 0), iota((384, 384), 1)
    return (row == (col % LANES) * STEPS + col // LANES).astype(BF)


def decay_rows(forget, pick):
    rows = jnp.concatenate([forget[p] for p in range(4)], axis=0)
    high = rows.astype(BF)
    rest = rows - high.astype(F32)
    middle = rest.astype(BF)
    low = (rest - middle.astype(F32)).astype(BF)
    parts = jnp.concatenate([high.astype(F32), middle.astype(F32), low.astype(F32)], axis=0).astype(BF)
    turned = lax.dot_general(pick, parts, NT, preferred_element_type=F32).astype(BF)
    row, col = iota((24, STATES), 0), iota((24, STATES), 1)
    group = jnp.where(col < 256, 2 * (col // 64), 2 * ((col - 256) // 32) + 1)
    place = (row % 8 == group).astype(BF)
    return jnp.exp(-jnp.dot(turned, place, preferred_element_type=F32))


def chain(first, ends, decay, run_base):
    now, starts = first, []
    for run in range(LANES):
        starts.append(now)
        part = slice(run, run + 1)
        grown = times(run_base, now)
        now = (
            decay[part] * grown[0] + ends[0][part],
            decay[part] * grown[1] + ends[1][part],
        )
    return [jnp.concatenate([s[i] for s in starts], axis=0) for i in range(2)], now


OFFSETS = (0, -1, 1, -2, 2, -3, 3, 4)
RIGHTWARD = (0, 1, 4, 5)
CHUNKS = ((0, 1, 2), (3, 4), (5, 6), (7,))
DIRECT = (2, 3)
COPY, DELAY, ISSUE, AHEAD = 0.703, 2.2, 0.03, 2.5
DUE = (32.0, 36.0, 42.0, 46.0)


def chunk_of(s):
    return [n for n, chunk in enumerate(CHUNKS) if s in chunk][0]


def slack(op):
    kind, n, s, hop = op
    step = DELAY + COPY
    if kind == "first":
        return (0.0 if n < 2 else 8.0) + hop
    if n < 2:
        return 15.0 - (4 - hop) * step
    if n == 3:
        return DUE[chunk_of(s)] - (4 - hop) * step
    return min(DUE[h - 1] - (h - hop) * step for h in range(hop, 5))


def waits_of(n, chunk=None):
    ops = []
    if chunk is None or chunk == 0:
        ops += [("first", n, 0, hop) for hop in range(1, 5)]
    for s in range(8):
        for hop in range(1, 5):
            mine = chunk is None or (hop == chunk + 1 if n == 2 else chunk_of(s) == chunk)
            if mine:
                ops.append(("line", n, s, hop))
    return set(ops)


def steps_of():
    ups = waits_of(0) | waits_of(1)
    steps = {
        "ywait": ((), 4.3, 0.1, set()),
        "zwait": (("ywait",), 4.5, 0.1, set()),
        "readout": (("zwait",), 0.0, 1.3, set()),
        "mats0": ((), 8.5, 0.05, set()),
        "mats1": (("mats0",), 5.6, 0.05, set()),
        "act": (("readout", "mats1"), 3.5, 0.2, set()),
        "mats2": (("mats1",), 5.0, 0.05, set()),
        "proj": (("act", "mats2"), 1.3, 1.0, set()),
        "rows0": (("proj",), 4.3, 0.05, set()),
        "rows1": (("rows0",), 2.1, 0.05, set()),
        "rows2": (("rows1",), 2.1, 0.05, set()),
        "up": (("rows2",), 1.3, 1.8, ups),
    }
    for c, chunk in enumerate(CHUNKS):
        width = len(chunk)
        needs = waits_of(2, c) | waits_of(3, c)
        steps[f"product{c}"] = (("up",) if c == 0 else ("up", f"product{c - 1}"), 0.0, 0.35 * width, needs)
        steps[f"sum{c}"] = ((f"product{c}",), 1.3 + 0.2 * width, 0.1, set())
        final = c in DIRECT
        if not final:
            steps[f"on{c}"] = ((f"sum{c}",), 2.4 + 0.5 * width, 0.1, set())
        steps[f"done{c}"] = ((f"sum{c}" if final else f"on{c}",), (3.2 + 1.0 * width) if final else 2.8 + 0.5 * width, 0.1, set())
        steps[f"pass{c}"] = ((f"done{c}",), 3.2 + 1.0 * width if final else 2.8 + 0.5 * width, 0.05, set())
        if not final:
            steps[f"last{c}"] = ((f"pass{c}",), 2.4 + 0.3 * width, 0.05, set())
        steps[f"out{c}"] = ((f"pass{c}" if final else f"last{c}",), 1.2, 0.05, set())
    steps["clean"] = ((f"product{len(CHUNKS) - 1}",), 0.1, 0.2, set())
    return steps


def plan():
    steps, order = steps_of(), []
    free, ready, coming = [1.0, 0.0], [set(), set()], []
    ended, seen, now = {}, set(), 0.0

    def link(op):
        return (op[1] + (op[0] == "line")) % 2

    def offer(op):
        ready[link(op)].add(op)

    for n in range(4):
        offer(("first", n, 0, 1))
        offer(("line", n, 0, 1))
    while steps or coming or ready[0] or ready[1]:
        for side in range(2):
            ahead = AHEAD
            for name, (before, after, own, needs) in steps.items():
                if own > 0.9 and all(b in ended for b in before) and needs <= seen:
                    if max([ended[b] for b in before], default=0.0) + after < now + 0.3:
                        ahead = AHEAD + own
            while ready[side] and free[side] - now < ahead:
                op = min(ready[side], key=lambda o: (slack(o), o))
                ready[side].remove(op)
                order.append(("send", op))
                both = 1.0 if op[3] < 4 else 0.5
                free[side] = max(free[side], now) + COPY * both
                coming.append((free[side] + DELAY, op))
                now += ISSUE
        due = min(coming, default=None)
        able = [
            (max([ended[b] for b in before], default=0.0) + after, name)
            for name, (before, after, _, needs) in steps.items()
            if all(b in ended for b in before) and needs <= seen
        ]
        step = min(able, default=None)
        if due and due[0] <= now or (due and (step is None or due[0] < step[0])):
            now = max(now, due[0]) + ISSUE
            coming.remove(due)
            op = due[1]
            seen.add(op)
            order.append(("wait", op))
            kind, n, s, hop = op
            if hop < 4:
                offer((kind, n, s, hop + 1))
            if kind == "first":
                for k, offset in enumerate(OFFSETS):
                    if abs(offset) == hop:
                        offer(("line", n, k, 1))
        elif step:
            wake = [free[side] - AHEAD * 0.5 for side in range(2) if ready[side]]
            if wake and min(wake) < step[0] and min(wake) > now:
                now = min(wake)
                continue
            now = max(now, step[0]) + steps[step[1]][2]
            ended[step[1]] = now
            order.append(("step", step[1]))
            if step[1] == "ywait":
                free[1] = max(free[1], now) + 1.0
            del steps[step[1]]
        else:
            now = max(now, min(free[side] for side in range(2) if ready[side]) - AHEAD * 0.5)
    return order, ended, now


def kernel(
    hidden_in, drive, wide_poles, narrow_poles, log_step, forget, wide_input, narrow_input,
    wide_output, narrow_output, skip, mix_gain, out_weight, mlp_gain, up_weight, down_weight,
    out,
    up_a, up_b, dn_a, dn_b, mats, normed, own_in, carried,
    push_r, push_i, decay, ymsg, zmsg, gains, act_out, act_in, squared,
    loc_sem, w_send, s1_recv, s2_recv, m_send, m_recv, ag_send, ag_recv, t_send, t_recv, out_sem,
    *pieces,
):
    part, pair_in, acc, half_in, side_in, final = (pieces[n :: 6] for n in range(6))
    sp, tp = lax.axis_index("sp"), lax.axis_index("tp")
    y, z, x, core = sp % 8, sp // 8, tp // 2, tp % 2

    def along_y(step):
        return z * 8 + (y + step + 8) % 8, tp

    def along_z(step):
        return ((z + step + 8) % 8) * 8 + y, tp

    def group(step):
        return sp, (tp + step) % 8

    def along_x(step):
        return sp, ((x + step + 4) % 4) * 2 + core

    partner = (sp, 2 * x + 1 - core)

    def send(src, dst, send_sem, recv_sem, to):
        pltpu.make_async_remote_copy(
            src_ref=src, dst_ref=dst, send_sem=send_sem, recv_sem=recv_sem, device_id=to, device_id_type=MESH
        ).start()

    def held(ref, sem):
        return pltpu.make_async_remote_copy(
            src_ref=ref, dst_ref=ref, send_sem=sem, recv_sem=sem, device_id=partner, device_id_type=MESH
        )

    def arrived(dst, recv_sem):
        held(dst, recv_sem).wait_recv()

    def left(src, send_sem):
        held(src, send_sem).wait_send()

    barrier = pltpu.get_barrier_semaphore()
    for step in range(1, 8):
        for to in (along_y(step), along_z(step), group(step)):
            pl.semaphore_signal(barrier, inc=1, device_id=to, device_id_type=MESH)
    bufs = (up_a, up_b, dn_a, dn_b)

    def where_of(n):
        return (y, z, along_y, along_z) if n % 2 == 0 else (z, y, along_z, along_y)

    def shard(n, first, second):
        return bufs[n].at[second * 8 + first]

    def mod8(v):
        return (v + 8) % 8

    local = []
    for n, weight in enumerate((up_weight, up_weight, down_weight, down_weight)):
        at, line, _, _ = where_of(n)
        local.append(
            pltpu.make_async_copy(weight.at[:, pl.ds((n % 2) * 512, 512)], shard(n, at, line), loc_sem.at[n])
        )
    local.append(pltpu.make_async_copy(out_weight, mats.at[tp], loc_sem.at[4]))
    local.append(pltpu.make_async_copy(hidden_in.at[pl.ds(pl.multiple_of(tp * 48, 16), 48)], own_in, loc_sem.at[5]))
    for copy in local:
        copy.start()
    def first_send(n, hop):
        at, line, go, _ = where_of(n)
        for direction in (1, -1) if hop < 4 else (1,):
            ref = shard(n, mod8(at - direction * (hop - 1)), line)
            send(ref, ref, w_send.at[n], s1_recv.at[n, hop - 1], go(direction))

    def line_send(n, s, hop):
        at, line, _, go = where_of(n)
        for direction in (1, -1):
            if hop < 4 or (s in RIGHTWARD) == (direction > 0):
                ref = shard(n, mod8(at + OFFSETS[s]), mod8(line - direction * (hop - 1)))
                send(ref, ref, w_send.at[n], s2_recv.at[n, 4 * s + hop - 1], go(direction))

    def copy_send(op):
        kind, n, s, hop = op
        if kind == "first":
            first_send(n, hop)
        else:
            line_send(n, s, hop)

    def copy_wait(op):
        kind, n, s, hop = op
        sem = s1_recv.at[n, hop - 1] if kind == "first" else s2_recv.at[n, 4 * s + hop - 1]
        arrived(bufs[n].at[pl.ds(0, 2 if hop < 4 else 1)], sem)

    halves = (pl.ds(0, 1024), pl.ds(1024, 1024))

    def gather_start(buf, g):
        ref = buf.at[tp]
        for turn in range(2):
            for n, direction in enumerate((1, -1)):
                half = (n + turn) % 2
                piece = ref.at[:, halves[half]]
                send(piece, piece, ag_send.at[g], ag_recv.at[g, 2 * n + turn], along_x(direction))
        send(ref, ref, ag_send.at[g], ag_recv.at[g, 6], partner)

    def gather_middle(buf, g, turns=(0, 1)):
        for turn in turns:
            for n, direction in enumerate((1, -1)):
                half = (n + turn) % 2
                piece = buf.at[along_x(-direction)[1], :, halves[half]]
                arrived(piece, ag_recv.at[g, 2 * n + turn])
                if turn == 0:
                    send(piece, piece, ag_send.at[g], ag_recv.at[g, 4 + n], along_x(direction))
                send(piece, piece, ag_send.at[g], ag_recv.at[g, 6], partner)

    def gather_end(buf, g):
        far = buf.at[along_x(2)[1]]
        for n in range(2):
            piece = far.at[:, halves[n]]
            arrived(piece, ag_recv.at[g, 4 + n])
            send(piece, piece, ag_send.at[g], ag_recv.at[g, 6], partner)

    def gather_partner(buf, g):
        arrived(buf.at[pl.ds(0, 4)], ag_recv.at[g, 6])

    def message(buf, at, state, fade):
        buf[at] = jnp.concatenate([state[0], state[1], fade, fade], axis=0)

    pick = order()
    decay[...] = decay_rows(forget, pick)
    drive_now = jnp.dot(pick, drive[...], preferred_element_type=F32).astype(BF)
    base, coef = discretize(wide_poles, narrow_poles, log_step)
    weights = [b.astype(BF) for b in blocks(wide_input, narrow_input)]
    pushed = times(coef, [jnp.dot(drive_now, w, preferred_element_type=F32) for w in weights])
    push_r[...] = pushed[0]
    push_i[...] = pushed[1]
    wide_base = [jnp.broadcast_to(b, (LANES, STATES)) for b in base]

    def scan_step(step, state):
        rows = pl.ds(pl.multiple_of(step * LANES, LANES), LANES)
        fade = decay[rows]
        grown = times(wide_base, state[:2])
        new = fade * grown[0] + push_r[rows], fade * grown[1] + push_i[rows], fade * state[2]
        push_r[rows], push_i[rows], decay[rows] = new
        return new

    zero = jnp.zeros((LANES, STATES), F32)
    end_r, end_i, total = lax.fori_loop(0, STEPS, scan_step, (zero, zero, zero + 1.0), unroll=4)
    powers = [base]
    for _ in range(5):
        powers.append(times(powers[-1], powers[-1]))
    run_base = times(powers[5], powers[4])
    _, last = chain((zero[:1], zero[:1]), (end_r, end_i), total, run_base)
    fade_all = total[:1]
    for run in range(1, LANES):
        fade_all = fade_all * total[run : run + 1]
    device_base = run_base
    for _ in range(3):
        device_base = times(device_base, device_base)
    line_base = device_base
    for _ in range(3):
        line_base = times(line_base, line_base)

    for copy in local:
        copy.wait()
    pl.semaphore_wait(barrier, 21)

    message(ymsg, y, last, fade_all)
    for step in range(1, 8):
        send(ymsg.at[y], ymsg.at[y], m_send.at[1], m_recv.at[1], along_y(step))
    held_values = {}

    def start_rest():
        gather_start(mats, 0)
        gains[tp] = mix_gain[...]
        for step in range(1, 8):
            send(mix_gain, gains.at[tp], m_send.at[0], m_recv.at[0], group(step))

    def do_ywait():
        arrived(ymsg.at[pl.ds(0, 7)], m_recv.at[1])
        zrow, onerow = zero[:1], zero[:1] + 1.0
        whole, before = (zrow, zrow), (zrow, zrow)
        whole_fade, before_fade, before_base = onerow, onerow, (onerow, zrow)
        for k in range(8):
            got = ymsg[k]
            fade = got[2:3]
            grown = times(device_base, whole)
            new = fade * grown[0] + got[0:1], fade * grown[1] + got[1:2]
            new_fade = whole_fade * fade
            new_base = times(before_base, device_base)
            earlier = k < y
            before = [jnp.where(earlier, n, o) for n, o in zip(new, before)]
            before_fade = jnp.where(earlier, new_fade, before_fade)
            before_base = [jnp.where(earlier, n, o) for n, o in zip(new_base, before_base)]
            whole, whole_fade = new, new_fade

        message(zmsg, z, whole, whole_fade)
        for step in range(1, 8):
            send(zmsg.at[z], zmsg.at[z], m_send.at[2], m_recv.at[2], along_z(step))
        held_values["before"] = before, before_fade, before_base

    def do_zwait():
        arrived(zmsg.at[pl.ds(0, 7)], m_recv.at[2])
        before, before_fade, before_base = held_values["before"]
        zrow = zero[:1]
        enter = (zrow, zrow)
        for k in range(8):
            got = zmsg[k]
            grown = times(line_base, enter)
            new = got[2:3] * grown[0] + got[0:1], got[2:3] * grown[1] + got[1:2]
            enter = [jnp.where(k < z, n, o) for n, o in zip(new, enter)]
        grown = times(before_base, enter)
        enter = before_fade * grown[0] + before[0], before_fade * grown[1] + before[1]

        held_values["enter"] = enter

    def do_readout():
        enter = held_values["enter"]
        starts, _ = chain(enter, (end_r, end_i), total, run_base)

        def fix_step(step, state):
            rows = pl.ds(pl.multiple_of(step * LANES, LANES), LANES)
            state = times(wide_base, state)
            push_r[rows] = push_r[rows] + decay[rows] * state[0]
            push_i[rows] = push_i[rows] + decay[rows] * state[1]
            return state

        lax.fori_loop(0, STEPS, fix_step, tuple(starts), unroll=4)
        real_block, imag_block = blocks(wide_output, narrow_output)
        response = lax.dot_general(push_r[...].astype(BF), real_block.astype(BF), NT, preferred_element_type=F32)
        response -= lax.dot_general(push_i[...].astype(BF), imag_block.astype(BF), NT, preferred_element_type=F32)
        response += skip[...] * drive_now.astype(F32)
        active = 0.5 * response * (1.0 + lax.erf(response * (0.5**0.5)))
        active = jnp.dot(back_order(), active.astype(BF), preferred_element_type=F32).astype(BF)

        act_out[...] = active.reshape(8, 48, 128)
        act_in[tp] = act_out[tp]
        for step in range(1, 8):
            to = group(step)
            send(act_out.at[to[1]], act_in.at[tp], m_send.at[3], m_recv.at[3], to)

    def do_act():
        arrived(gains.at[pl.ds(0, 7)], m_recv.at[0])
        arrived(act_in.at[pl.ds(0, 7)], m_recv.at[3])
        rows = jnp.concatenate([act_in[k] for k in range(8)], axis=1).astype(F32)
        gain = jnp.concatenate([gains[k] for k in range(8)], axis=1)
        power = jnp.sum(rows * rows, axis=1, keepdims=True) * (1.0 / 1024)
        held_values["mixed"] = (rows * lax.rsqrt(power + EPS) * gain).astype(BF)

    def do_proj():
        gather_partner(mats, 0)
        for n in range(8):
            cols = pl.ds(n * 256, 256)
            proj = jnp.dot(held_values["mixed"], mats[:, :, cols].reshape(1024, 256), preferred_element_type=F32)
            carried[:, cols] = (own_in[:, cols].astype(F32) + proj).astype(BF)
        values = carried[...].astype(F32)
        power = jnp.sum(values * values, axis=1, keepdims=True) * (1.0 / 2048)
        normed[tp] = (values * lax.rsqrt(power + EPS) * mlp_gain[...]).astype(BF)
        gather_start(normed, 1)

    def do_up():
        gather_partner(normed, 1)
        for n in range(4):
            cols = pl.ds((n % 2) * 256, 256)
            buf = bufs[n // 2]
            if n < 2:
                weight = buf[:, :, cols].reshape(2048, 256)
            else:
                weight = jnp.concatenate([buf[(s % 8) * 8 + s // 8, :, cols] for s in range(64)], axis=0)
            pre = jnp.dot(normed[...].reshape(384, 2048), weight, preferred_element_type=F32)
            pre = jnp.maximum(pre, 0.0)
            squared[:, pl.ds(n * 256, 256)] = (pre * pre).astype(BF)

    def chip(step):
        return (x + step + 4) % 4

    def halves_of(c):
        half = len(CHUNKS[c]) * 128
        return pl.ds(0, half), pl.ds(half, half)

    def unit(c, k):
        return mod8(z + OFFSETS[CHUNKS[c][k]])

    def do_product(c):
        for k in range(len(CHUNKS[c])):
            q = unit(c, k)
            first = dn_a[pl.ds(pl.multiple_of(q * 8, 8), 8)].reshape(256, 512)
            second = jnp.concatenate([dn_b[s * 8 + q] for s in range(8)], axis=0)
            piece = lax.dot_general(squared[:, :512], first, NT, preferred_element_type=F32)
            piece += lax.dot_general(squared[:, 512:], second, NT, preferred_element_type=F32)
            piece = piece.astype(BF)
            for b in range(8):
                part[c][(b % 2) * 4 + b // 2, :, pl.ds(k * 256, 256)] = piece[b * 48 : (b + 1) * 48]
        send(part[c].at[pl.ds((1 - core) * 4, 4)], pair_in[c], t_send.at[c], t_recv.at[c, 0], partner)

    def chip_sum(c, step, cols=slice(None)):
        at = chip(step)
        return part[c][core * 4 + at, :, cols].astype(F32) + pair_in[c][at, :, cols].astype(F32)

    def do_sum(c):
        arrived(pair_in[c], t_recv.at[c, 0])
        if c in DIRECT:
            for n, step in enumerate((2, 1, -1)):
                acc[c][n] = chip_sum(c, step).astype(BF)
                send(acc[c].at[n], side_in[c].at[n], t_send.at[c], t_recv.at[c, 3], along_x(step))
            return
        cut = halves_of(c)
        acc[c][0] = chip_sum(c, 2).astype(BF)
        for n, direction in enumerate((1, -1)):
            send(acc[c].at[0, :, cut[n]], half_in[c].at[n], t_send.at[c], t_recv.at[c, 1 + n], along_x(direction))
        for n, direction in enumerate((1, -1)):
            ready = cut[1 - n]
            acc[c][1 + n, :, ready] = chip_sum(c, direction, ready).astype(BF)
            send(
                acc[c].at[1 + n, :, ready], side_in[c].at[n, :, ready],
                t_send.at[c], t_recv.at[c, 3], along_x(direction),
            )

    def do_on(c):
        cut = halves_of(c)
        for n, direction in enumerate((1, -1)):
            arrived(half_in[c].at[n], t_recv.at[c, 1 + n])
            acc[c][1 + n, :, cut[n]] = (chip_sum(c, direction, cut[n]) + half_in[c][n].astype(F32)).astype(BF)
            send(
                acc[c].at[1 + n, :, cut[n]], side_in[c].at[n, :, cut[n]],
                t_send.at[c], t_recv.at[c, 3], along_x(direction),
            )

    def do_done(c):
        cols = [carried[:, pl.ds(pl.multiple_of(unit(c, k) * 256, 256), 256)] for k in range(len(CHUNKS[c]))]
        mine = chip_sum(c, 0) + jnp.concatenate(cols, axis=1).astype(F32)
        arrived(side_in[c], t_recv.at[c, 3])
        for n in range(3 if c in DIRECT else 2):
            mine += side_in[c][n].astype(F32)
        final[c][tp] = mine.astype(BF)
        ref = final[c].at[tp]
        for n, step in enumerate((1, -1, 2) if c in DIRECT else (1, -1)):
            send(ref, ref, t_send.at[c], t_recv.at[c, 4 + n], along_x(step))
        send(ref, ref, t_send.at[c], t_recv.at[c, 8], partner)

    def do_pass(c):
        for n, step in enumerate((1, -1, 2) if c in DIRECT else (1, -1)):
            ref = final[c].at[along_x(-step)[1]]
            arrived(ref, t_recv.at[c, 4 + n])
            if c not in DIRECT:
                piece = ref.at[:, halves_of(c)[n]]
                send(piece, piece, t_send.at[c], t_recv.at[c, 6 + n], along_x(step))
            send(ref, ref, t_send.at[c], t_recv.at[c, 8], partner)

    def do_last(c):
        for n in range(2):
            piece = final[c].at[along_x(2)[1], :, halves_of(c)[n]]
            arrived(piece, t_recv.at[c, 6 + n])
            send(piece, piece, t_send.at[c], t_recv.at[c, 8], partner)

    def out_copy(c, k):
        cols = pl.ds(pl.multiple_of(unit(c, k) * 256, 256), 256)
        return pltpu.make_async_copy(
            final[c].at[:, :, pl.ds(k * 256, 256)], out.at[:, :, cols], out_sem.at[CHUNKS[c][k]]
        )

    def do_out(c):
        arrived(final[c].at[pl.ds(0, 4)], t_recv.at[c, 8])
        for k in range(len(CHUNKS[c])):
            out_copy(c, k).start()

    def do_clean():
        for n in range(4):
            left(bufs[n].at[pl.ds(0, 63)], w_send.at[n])
        left(gains.at[pl.ds(0, 7)], m_send.at[0])
        left(ymsg.at[pl.ds(0, 7)], m_send.at[1])
        left(zmsg.at[pl.ds(0, 7)], m_send.at[2])
        left(act_out.at[pl.ds(0, 7)], m_send.at[3])
        left(mats.at[pl.ds(0, 7)], ag_send.at[0])
        left(normed.at[pl.ds(0, 7)], ag_send.at[1])

    do = {
        "ywait": do_ywait, "zwait": do_zwait, "readout": do_readout, "act": do_act, "proj": do_proj, "up": do_up,
        "clean": do_clean,
        "mats0": lambda: gather_middle(mats, 0, (0,)), "mats1": lambda: gather_middle(mats, 0, (1,)),
        "mats2": lambda: gather_end(mats, 0),
        "rows0": lambda: gather_middle(normed, 1, (0,)), "rows1": lambda: gather_middle(normed, 1, (1,)),
        "rows2": lambda: gather_end(normed, 1),
    }
    by_chunk = {
        "product": do_product, "sum": do_sum, "on": do_on, "done": do_done, "pass": do_pass, "last": do_last,
        "out": do_out,
    }
    started = False
    for kind, what in plan()[0]:
        if kind == "wait" and not started:
            started = True
            start_rest()
        if kind == "send":
            copy_send(what)
        elif kind == "wait":
            copy_wait(what)
        else:
            if what in do:
                do[what]()
            else:
                by_chunk[what[:-1]](int(what[-1]))
    for c, chunk in enumerate(CHUNKS):
        for k in range(len(chunk)):
            out_copy(c, k).wait()
        left(part[c], t_send.at[c])


def step(*args):
    args = list(args)
    for n in (10, 11, 13):
        args[n] = args[n].reshape(1, -1)
    args[4] = args[4].T
    for n in (6, 7):
        args[n] = jnp.swapaxes(args[n], 2, 3)
    vmem, hbm = pl.BlockSpec(memory_space=pltpu.VMEM), pl.BlockSpec(memory_space=pltpu.HBM)
    dma = pltpu.SemaphoreType.DMA
    scratch = [
        *[pltpu.VMEM((64, 32, 512), BF)] * 4,
        pltpu.VMEM((8, 128, 2048), BF),
        pltpu.VMEM((8, 48, 2048), BF),
        pltpu.VMEM((48, 2048), BF),
        pltpu.VMEM((48, 2048), BF),
        *[pltpu.VMEM((384, STATES), F32)] * 3,
        *[pltpu.VMEM((8, 4, STATES), F32)] * 2,
        pltpu.VMEM((8, 1, 128), F32),
        pltpu.VMEM((8, 48, 128), BF),
        pltpu.VMEM((8, 48, 128), BF),
        pltpu.VMEM((384, 1024), BF),
        dma((6,)), dma((4,)), dma((4, 4)), dma((4, 32)), dma((4,)), dma((4,)),
        dma((2,)), dma((2, 7)), dma((4,)), dma((4, 9)), dma((8,)),
    ]
    for c, chunk in enumerate(CHUNKS):
        width = 256 * len(chunk)
        final = c in DIRECT
        scratch += [
            pltpu.VMEM((14, 48, width), BF),
            pltpu.VMEM((4, 48, width), BF),
            pltpu.VMEM((3, 48, width), BF),
            pltpu.VMEM((2, 48, width // 2), BF),
            pltpu.VMEM((3 if final else 2, 48, width), BF),
            pltpu.VMEM((8, 48, width), BF),
        ]
    whole = pl.pallas_call(
        kernel,
        out_shape=jax.ShapeDtypeStruct((8, 48, 2048), BF),
        in_specs=[hbm if n in (0, 12, 14, 15) else vmem for n in range(16)],
        out_specs=hbm,
        scratch_shapes=scratch,
        compiler_params=pltpu.CompilerParams(
            collective_id=0, has_side_effects=True, vmem_limit_bytes=58 * 1024 * 1024
        ),
    )(*args)
    return whole.reshape(384, 2048)


def solution(mesh):
    return jax.shard_map(
        step,
        mesh=mesh,
        in_specs=(
            P("sp", None),
            P("sp", "tp"),
            P(None, "tp", None),
            P(None, "tp", None),
            P("tp", None),
            P("tp", None, "sp"),
            P(None, "tp", None, None),
            P(None, "tp", None, None),
            P(None, "tp", None, None),
            P(None, "tp", None, None),
            P("tp"),
            P("tp"),
            P("tp", None),
            P(),
            P("sp", "tp"),
            P("sp", "tp"),
        ),
        out_specs=P("sp", None),
        check_vma=False,
    )
```

```python
import jax
import jax.numpy as jnp
from jax import lax
from jax.experimental import pallas as pl
from jax.experimental.pallas import tpu as pltpu
from jax.sharding import PartitionSpec as P

MESH = pl.DeviceIdType.MESH
BF, F32 = jnp.bfloat16, jnp.float32
EPS = 1e-06
NT = (((1,), (1,)), ((), ()))
STATES = 384
STEPS, LANES = 48, 8


def iota(shape, dim):
    return lax.broadcasted_iota(jnp.int32, shape, dim)


def one_row(values):
    rows, width = values.shape
    tiled = jnp.concatenate([values] * rows, axis=1)
    keep = iota(tiled.shape, 0) == iota(tiled.shape, 1) // width
    return jnp.sum(jnp.where(keep, tiled, 0.0), axis=0, keepdims=True)


def spread(line, width):
    keep = iota((4, 4), 0) == iota((4, 4), 1)
    column = jnp.sum(jnp.where(keep, jnp.broadcast_to(line, (4, 4)), 0.0), axis=1, keepdims=True)
    shape = (4, 4 * width)
    keep = iota(shape, 0) == iota(shape, 1) // width
    return jnp.sum(jnp.where(keep, jnp.broadcast_to(column, shape), 0.0), axis=0, keepdims=True)


def expm1_small(x):
    total = jnp.ones_like(x)
    for order in range(9, 1, -1):
        total = 1.0 + total * x * (1.0 / order)
    return total * x


def times(a, b):
    return a[0] * b[0] - a[1] * b[1], a[0] * b[1] + a[1] * b[0]


def discretize(wide_poles, narrow_poles, log_step):
    real = jnp.concatenate([one_row(wide_poles[0]), one_row(narrow_poles[0])], axis=1)
    imag = jnp.concatenate([one_row(wide_poles[1]), one_row(narrow_poles[1])], axis=1)
    steps = log_step[...]
    step = jnp.exp(jnp.concatenate([spread(steps[:1], 64), spread(steps[1:], 32)], axis=1))
    growth, angle = real * step, imag * step
    size, sine, cosine = jnp.exp(growth), jnp.sin(angle), jnp.cos(angle)
    half = jnp.sin(0.5 * angle)
    rise_real = expm1_small(growth) * cosine - 2.0 * half * half
    rise_imag = size * sine
    bottom = real * real + imag * imag
    coef_real = (rise_real * real + rise_imag * imag) / bottom
    coef_imag = (rise_imag * real - rise_real * imag) / bottom
    return (size * cosine, size * sine), (coef_real, coef_imag)


def blocks(first, second):
    out = []
    for part in range(2):
        halves = []
        for kind, (ref, width) in enumerate(((first, 64), (second, 32))):
            flat = ref[part].reshape(64, width)
            row, col = iota((128, 64), 0), iota((128, 64), 1)
            pick = ((row // 32 == col // 16) & (row % 16 == col % 16)).astype(BF)
            rows = jnp.dot(pick, flat, preferred_element_type=F32).astype(BF)
            repeat = (iota((width, 4 * width), 1) % width == iota((width, 4 * width), 0)).astype(BF)
            tiled = jnp.dot(rows, repeat, preferred_element_type=F32)
            row, col = iota(tiled.shape, 0), iota(tiled.shape, 1)
            keep = (row // 32 == col // width) & ((row // 16) % 2 == kind)
            halves.append(jnp.where(keep, tiled, 0.0))
        out.append(jnp.concatenate(halves, axis=1))
    return out


def order():
    row, col = iota((384, 384), 0), iota((384, 384), 1)
    return (col == (row % LANES) * STEPS + row // LANES).astype(BF)


def back_order():
    row, col = iota((384, 384), 0), iota((384, 384), 1)
    return (row == (col % LANES) * STEPS + col // LANES).astype(BF)


def decay_rows(forget, pick):
    rows = jnp.concatenate([forget[p] for p in range(4)], axis=0)
    high = rows.astype(BF)
    rest = rows - high.astype(F32)
    middle = rest.astype(BF)
    low = (rest - middle.astype(F32)).astype(BF)
    parts = jnp.concatenate([high.astype(F32), middle.astype(F32), low.astype(F32)], axis=0).astype(BF)
    turned = lax.dot_general(pick, parts, NT, preferred_element_type=F32).astype(BF)
    row, col = iota((24, STATES), 0), iota((24, STATES), 1)
    group = jnp.where(col < 256, 2 * (col // 64), 2 * ((col - 256) // 32) + 1)
    place = (row % 8 == group).astype(BF)
    return jnp.exp(-jnp.dot(turned, place, preferred_element_type=F32))


def chain(first, ends, decay, run_base):
    now, starts = first, []
    for run in range(LANES):
        starts.append(now)
        part = slice(run, run + 1)
        grown = times(run_base, now)
        now = (
            decay[part] * grown[0] + ends[0][part],
            decay[part] * grown[1] + ends[1][part],
        )
    return [jnp.concatenate([s[i] for s in starts], axis=0) for i in range(2)], now


OFFSETS = (0, -1, 1, -2, 2, -3, 3, 4)
RIGHTWARD = (0, 1, 4, 5)
CHUNKS = ((0, 1, 2), (3, 4), (5, 6), (7,))
DIRECT = (2, 3)
COPY, DELAY, ISSUE, AHEAD = 0.703, 2.2, 0.03, 2.5
DUE = (32.0, 36.0, 42.0, 46.0)


def chunk_of(s):
    return [n for n, chunk in enumerate(CHUNKS) if s in chunk][0]


def slack(op):
    kind, n, s, hop = op
    step = DELAY + COPY
    if kind == "first":
        return (0.0 if n < 2 else 8.0) + hop
    if n < 2:
        return 15.0 - (4 - hop) * step
    if n == 3:
        return DUE[chunk_of(s)] - (4 - hop) * step
    return min(DUE[h - 1] - (h - hop) * step for h in range(hop, 5))


def waits_of(n, chunk=None):
    ops = []
    if chunk is None or chunk == 0:
        ops += [("first", n, 0, hop) for hop in range(1, 5)]
    for s in range(8):
        for hop in range(1, 5):
            mine = chunk is None or (hop == chunk + 1 if n == 2 else chunk_of(s) == chunk)
            if mine:
                ops.append(("line", n, s, hop))
    return set(ops)


def steps_of():
    ups = waits_of(0) | waits_of(1)
    steps = {
        "ywait": ((), 4.3, 0.1, set()),
        "zwait": (("ywait",), 4.5, 0.1, set()),
        "readout": (("zwait",), 0.0, 1.3, set()),
        "mats0": ((), 8.5, 0.05, set()),
        "mats1": (("mats0",), 5.6, 0.05, set()),
        "act": (("readout", "mats1"), 3.5, 0.2, set()),
        "mats2": (("mats1",), 5.0, 0.05, set()),
        "proj": (("act", "mats2"), 1.3, 1.0, set()),
        "rows0": (("proj",), 4.3, 0.05, set()),
        "rows1": (("rows0",), 2.1, 0.05, set()),
        "rows2": (("rows1",), 2.1, 0.05, set()),
        "up": (("rows2",), 1.3, 1.8, ups),
    }
    for c, chunk in enumerate(CHUNKS):
        width = len(chunk)
        needs = waits_of(2, c) | waits_of(3, c)
        steps[f"product{c}"] = (("up",) if c == 0 else ("up", f"product{c - 1}"), 0.0, 0.35 * width, needs)
        steps[f"sum{c}"] = ((f"product{c}",), 1.3 + 0.2 * width, 0.1, set())
        final = c in DIRECT
        if not final:
            steps[f"on{c}"] = ((f"sum{c}",), 2.4 + 0.5 * width, 0.1, set())
        steps[f"done{c}"] = ((f"sum{c}" if final else f"on{c}",), (3.2 + 1.0 * width) if final else 2.8 + 0.5 * width, 0.1, set())
        steps[f"pass{c}"] = ((f"done{c}",), 3.2 + 1.0 * width if final else 2.8 + 0.5 * width, 0.05, set())
        if not final:
            steps[f"last{c}"] = ((f"pass{c}",), 2.4 + 0.3 * width, 0.05, set())
        steps[f"out{c}"] = ((f"pass{c}" if final else f"last{c}",), 1.2, 0.05, set())
    steps["clean"] = ((f"product{len(CHUNKS) - 1}",), 0.1, 0.2, set())
    return steps


def plan():
    steps, order = steps_of(), []
    free, ready, coming = [1.0, 0.0], [set(), set()], []
    ended, seen, now = {}, set(), 0.0

    def link(op):
        return (op[1] + (op[0] == "line")) % 2

    def offer(op):
        ready[link(op)].add(op)

    for n in range(4):
        offer(("first", n, 0, 1))
        offer(("line", n, 0, 1))
    while steps or coming or ready[0] or ready[1]:
        for side in range(2):
            ahead = AHEAD
            for name, (before, after, own, needs) in steps.items():
                if own > 0.9 and all(b in ended for b in before) and needs <= seen:
                    if max([ended[b] for b in before], default=0.0) + after < now + 0.3:
                        ahead = AHEAD + own
            while ready[side] and free[side] - now < ahead:
                op = min(ready[side], key=lambda o: (slack(o), o))
                ready[side].remove(op)
                order.append(("send", op))
                both = 1.0 if op[3] < 4 else 0.5
                free[side] = max(free[side], now) + COPY * both
                coming.append((free[side] + DELAY, op))
                now += ISSUE
        due = min(coming, default=None)
        able = [
            (max([ended[b] for b in before], default=0.0) + after, name)
            for name, (before, after, _, needs) in steps.items()
            if all(b in ended for b in before) and needs <= seen
        ]
        step = min(able, default=None)
        if due and due[0] <= now or (due and (step is None or due[0] < step[0])):
            now = max(now, due[0]) + ISSUE
            coming.remove(due)
            op = due[1]
            seen.add(op)
            order.append(("wait", op))
            kind, n, s, hop = op
            if hop < 4:
                offer((kind, n, s, hop + 1))
            if kind == "first":
                for k, offset in enumerate(OFFSETS):
                    if abs(offset) == hop:
                        offer(("line", n, k, 1))
        elif step:
            wake = [free[side] - AHEAD * 0.5 for side in range(2) if ready[side]]
            if wake and min(wake) < step[0] and min(wake) > now:
                now = min(wake)
                continue
            now = max(now, step[0]) + steps[step[1]][2]
            ended[step[1]] = now
            order.append(("step", step[1]))
            if step[1] == "ywait":
                free[1] = max(free[1], now) + 1.0
            del steps[step[1]]
        else:
            now = max(now, min(free[side] for side in range(2) if ready[side]) - AHEAD * 0.5)
    return order, ended, now


def kernel(
    hidden_in, drive, wide_poles, narrow_poles, log_step, forget, wide_input, narrow_input,
    wide_output, narrow_output, skip, mix_gain, out_weight, mlp_gain, up_weight, down_weight,
    out,
    up_a, up_b, dn_a, dn_b, mats, normed, own_in, carried,
    push_r, push_i, decay, ymsg, zmsg, gains, act_out, act_in, squared,
    loc_sem, w_send, s1_recv, s2_recv, m_send, m_recv, ag_send, ag_recv, t_send, t_recv, out_sem,
    *pieces,
):
    part, pair_in, acc, half_in, side_in, final = (pieces[n :: 6] for n in range(6))
    sp, tp = lax.axis_index("sp"), lax.axis_index("tp")
    y, z, x, core = sp % 8, sp // 8, tp // 2, tp % 2

    def along_y(step):
        return z * 8 + (y + step + 8) % 8, tp

    def along_z(step):
        return ((z + step + 8) % 8) * 8 + y, tp

    def group(step):
        return sp, (tp + step) % 8

    def along_x(step):
        return sp, ((x + step + 4) % 4) * 2 + core

    partner = (sp, 2 * x + 1 - core)

    def send(src, dst, send_sem, recv_sem, to):
        pltpu.make_async_remote_copy(
            src_ref=src, dst_ref=dst, send_sem=send_sem, recv_sem=recv_sem, device_id=to, device_id_type=MESH
        ).start()

    def held(ref, sem):
        return pltpu.make_async_remote_copy(
            src_ref=ref, dst_ref=ref, send_sem=sem, recv_sem=sem, device_id=partner, device_id_type=MESH
        )

    def arrived(dst, recv_sem):
        held(dst, recv_sem).wait_recv()

    def left(src, send_sem):
        held(src, send_sem).wait_send()

    barrier = pltpu.get_barrier_semaphore()
    for step in range(1, 8):
        for to in (along_y(step), along_z(step), group(step)):
            pl.semaphore_signal(barrier, inc=1, device_id=to, device_id_type=MESH)
    bufs = (up_a, up_b, dn_a, dn_b)

    def where_of(n):
        return (y, z, along_y, along_z) if n % 2 == 0 else (z, y, along_z, along_y)

    def shard(n, first, second):
        return bufs[n].at[second * 8 + first]

    def mod8(v):
        return (v + 8) % 8

    local = []
    for n, weight in enumerate((up_weight, up_weight, down_weight, down_weight)):
        at, line, _, _ = where_of(n)
        local.append(
            pltpu.make_async_copy(weight.at[:, pl.ds((n % 2) * 512, 512)], shard(n, at, line), loc_sem.at[n])
        )
    local.append(pltpu.make_async_copy(out_weight, mats.at[tp], loc_sem.at[4]))
    local.append(pltpu.make_async_copy(hidden_in.at[pl.ds(pl.multiple_of(tp * 48, 16), 48)], own_in, loc_sem.at[5]))
    for copy in local:
        copy.start()
    def first_send(n, hop):
        at, line, go, _ = where_of(n)
        for direction in (1, -1) if hop < 4 else (1,):
            ref = shard(n, mod8(at - direction * (hop - 1)), line)
            send(ref, ref, w_send.at[n], s1_recv.at[n, hop - 1], go(direction))

    def line_send(n, s, hop):
        at, line, _, go = where_of(n)
        for direction in (1, -1):
            if hop < 4 or (s in RIGHTWARD) == (direction > 0):
                ref = shard(n, mod8(at + OFFSETS[s]), mod8(line - direction * (hop - 1)))
                send(ref, ref, w_send.at[n], s2_recv.at[n, 4 * s + hop - 1], go(direction))

    def copy_send(op):
        kind, n, s, hop = op
        if kind == "first":
            first_send(n, hop)
        else:
            line_send(n, s, hop)

    def copy_wait(op):
        kind, n, s, hop = op
        sem = s1_recv.at[n, hop - 1] if kind == "first" else s2_recv.at[n, 4 * s + hop - 1]
        arrived(bufs[n].at[pl.ds(0, 2 if hop < 4 else 1)], sem)

    halves = (pl.ds(0, 1024), pl.ds(1024, 1024))

    def gather_start(buf, g):
        ref = buf.at[tp]
        for turn in range(2):
            for n, direction in enumerate((1, -1)):
                half = (n + turn) % 2
                piece = ref.at[:, halves[half]]
                send(piece, piece, ag_send.at[g], ag_recv.at[g, 2 * n + turn], along_x(direction))
        send(ref, ref, ag_send.at[g], ag_recv.at[g, 6], partner)

    def gather_middle(buf, g, turns=(0, 1)):
        for turn in turns:
            for n, direction in enumerate((1, -1)):
                half = (n + turn) % 2
                piece = buf.at[along_x(-direction)[1], :, halves[half]]
                arrived(piece, ag_recv.at[g, 2 * n + turn])
                if turn == 0:
                    send(piece, piece, ag_send.at[g], ag_recv.at[g, 4 + n], along_x(direction))
                send(piece, piece, ag_send.at[g], ag_recv.at[g, 6], partner)

    def gather_end(buf, g):
        far = buf.at[along_x(2)[1]]
        for n in range(2):
            piece = far.at[:, halves[n]]
            arrived(piece, ag_recv.at[g, 4 + n])
            send(piece, piece, ag_send.at[g], ag_recv.at[g, 6], partner)

    def gather_partner(buf, g):
        arrived(buf.at[pl.ds(0, 4)], ag_recv.at[g, 6])

    def message(buf, at, state, fade):
        buf[at] = jnp.concatenate([state[0], state[1], fade, fade], axis=0)

    pick = order()
    decay[...] = decay_rows(forget, pick)
    drive_now = jnp.dot(pick, drive[...], preferred_element_type=F32).astype(BF)
    base, coef = discretize(wide_poles, narrow_poles, log_step)
    weights = [b.astype(BF) for b in blocks(wide_input, narrow_input)]
    pushed = times(coef, [jnp.dot(drive_now, w, preferred_element_type=F32) for w in weights])
    push_r[...] = pushed[0]
    push_i[...] = pushed[1]
    wide_base = [jnp.broadcast_to(b, (LANES, STATES)) for b in base]

    def scan_step(step, state):
        rows = pl.ds(pl.multiple_of(step * LANES, LANES), LANES)
        fade = decay[rows]
        grown = times(wide_base, state[:2])
        new = fade * grown[0] + push_r[rows], fade * grown[1] + push_i[rows], fade * state[2]
        push_r[rows], push_i[rows], decay[rows] = new
        return new

    zero = jnp.zeros((LANES, STATES), F32)
    end_r, end_i, total = lax.fori_loop(0, STEPS, scan_step, (zero, zero, zero + 1.0), unroll=4)
    powers = [base]
    for _ in range(5):
        powers.append(times(powers[-1], powers[-1]))
    run_base = times(powers[5], powers[4])
    _, last = chain((zero[:1], zero[:1]), (end_r, end_i), total, run_base)
    fade_all = total[:1]
    for run in range(1, LANES):
        fade_all = fade_all * total[run : run + 1]
    device_base = run_base
    for _ in range(3):
        device_base = times(device_base, device_base)
    line_base = device_base
    for _ in range(3):
        line_base = times(line_base, line_base)

    for copy in local:
        copy.wait()
    pl.semaphore_wait(barrier, 21)

    message(ymsg, y, last, fade_all)
    for step in range(1, 8):
        send(ymsg.at[y], ymsg.at[y], m_send.at[1], m_recv.at[1], along_y(step))
    held_values = {}

    def start_rest():
        gather_start(mats, 0)
        gains[tp] = mix_gain[...]
        for step in range(1, 8):
            send(mix_gain, gains.at[tp], m_send.at[0], m_recv.at[0], group(step))

    def do_ywait():
        arrived(ymsg.at[pl.ds(0, 7)], m_recv.at[1])
        zrow, onerow = zero[:1], zero[:1] + 1.0
        whole, before = (zrow, zrow), (zrow, zrow)
        whole_fade, before_fade, before_base = onerow, onerow, (onerow, zrow)
        for k in range(8):
            got = ymsg[k]
            fade = got[2:3]
            grown = times(device_base, whole)
            new = fade * grown[0] + got[0:1], fade * grown[1] + got[1:2]
            new_fade = whole_fade * fade
            new_base = times(before_base, device_base)
            earlier = k < y
            before = [jnp.where(earlier, n, o) for n, o in zip(new, before)]
            before_fade = jnp.where(earlier, new_fade, before_fade)
            before_base = [jnp.where(earlier, n, o) for n, o in zip(new_base, before_base)]
            whole, whole_fade = new, new_fade

        message(zmsg, z, whole, whole_fade)
        for step in range(1, 8):
            send(zmsg.at[z], zmsg.at[z], m_send.at[2], m_recv.at[2], along_z(step))
        held_values["before"] = before, before_fade, before_base

    def do_zwait():
        arrived(zmsg.at[pl.ds(0, 7)], m_recv.at[2])
        before, before_fade, before_base = held_values["before"]
        zrow = zero[:1]
        enter = (zrow, zrow)
        for k in range(8):
            got = zmsg[k]
            grown = times(line_base, enter)
            new = got[2:3] * grown[0] + got[0:1], got[2:3] * grown[1] + got[1:2]
            enter = [jnp.where(k < z, n, o) for n, o in zip(new, enter)]
        grown = times(before_base, enter)
        enter = before_fade * grown[0] + before[0], before_fade * grown[1] + before[1]

        held_values["enter"] = enter

    def do_readout():
        enter = held_values["enter"]
        starts, _ = chain(enter, (end_r, end_i), total, run_base)

        def fix_step(step, state):
            rows = pl.ds(pl.multiple_of(step * LANES, LANES), LANES)
            state = times(wide_base, state)
            push_r[rows] = push_r[rows] + decay[rows] * state[0]
            push_i[rows] = push_i[rows] + decay[rows] * state[1]
            return state

        lax.fori_loop(0, STEPS, fix_step, tuple(starts), unroll=4)
        real_block, imag_block = blocks(wide_output, narrow_output)
        response = lax.dot_general(push_r[...].astype(BF), real_block.astype(BF), NT, preferred_element_type=F32)
        response -= lax.dot_general(push_i[...].astype(BF), imag_block.astype(BF), NT, preferred_element_type=F32)
        response += skip[...] * drive_now.astype(F32)
        active = 0.5 * response * (1.0 + lax.erf(response * (0.5**0.5)))
        active = jnp.dot(back_order(), active.astype(BF), preferred_element_type=F32).astype(BF)

        act_out[...] = active.reshape(8, 48, 128)
        act_in[tp] = act_out[tp]
        for step in range(1, 8):
            to = group(step)
            send(act_out.at[to[1]], act_in.at[tp], m_send.at[3], m_recv.at[3], to)

    def do_act():
        arrived(gains.at[pl.ds(0, 7)], m_recv.at[0])
        arrived(act_in.at[pl.ds(0, 7)], m_recv.at[3])
        rows = jnp.concatenate([act_in[k] for k in range(8)], axis=1).astype(F32)
        gain = jnp.concatenate([gains[k] for k in range(8)], axis=1)
        power = jnp.sum(rows * rows, axis=1, keepdims=True) * (1.0 / 1024)
        held_values["mixed"] = (rows * lax.rsqrt(power + EPS) * gain).astype(BF)

    def do_proj():
        gather_partner(mats, 0)
        for n in range(8):
            cols = pl.ds(n * 256, 256)
            proj = jnp.dot(held_values["mixed"], mats[:, :, cols].reshape(1024, 256), preferred_element_type=F32)
            carried[:, cols] = (own_in[:, cols].astype(F32) + proj).astype(BF)
        values = carried[...].astype(F32)
        power = jnp.sum(values * values, axis=1, keepdims=True) * (1.0 / 2048)
        normed[tp] = (values * lax.rsqrt(power + EPS) * mlp_gain[...]).astype(BF)
        gather_start(normed, 1)

    def do_up():
        gather_partner(normed, 1)
        for n in range(4):
            cols = pl.ds((n % 2) * 256, 256)
            buf = bufs[n // 2]
            if n < 2:
                weight = buf[:, :, cols].reshape(2048, 256)
            else:
                weight = jnp.concatenate([buf[(s % 8) * 8 + s // 8, :, cols] for s in range(64)], axis=0)
            pre = jnp.dot(normed[...].reshape(384, 2048), weight, preferred_element_type=F32)
            pre = jnp.maximum(pre, 0.0)
            squared[:, pl.ds(n * 256, 256)] = (pre * pre).astype(BF)

    def chip(step):
        return (x + step + 4) % 4

    def halves_of(c):
        half = len(CHUNKS[c]) * 128
        return pl.ds(0, half), pl.ds(half, half)

    def unit(c, k):
        return mod8(z + OFFSETS[CHUNKS[c][k]])

    def do_product(c):
        for k in range(len(CHUNKS[c])):
            q = unit(c, k)
            first = dn_a[pl.ds(pl.multiple_of(q * 8, 8), 8)].reshape(256, 512)
            second = jnp.concatenate([dn_b[s * 8 + q] for s in range(8)], axis=0)
            piece = lax.dot_general(squared[:, :512], first, NT, preferred_element_type=F32)
            piece += lax.dot_general(squared[:, 512:], second, NT, preferred_element_type=F32)
            piece = piece.astype(BF)
            for b in range(8):
                part[c][(b % 2) * 4 + b // 2, :, pl.ds(k * 256, 256)] = piece[b * 48 : (b + 1) * 48]
        send(part[c].at[pl.ds((1 - core) * 4, 4)], pair_in[c], t_send.at[c], t_recv.at[c, 0], partner)

    def chip_sum(c, step, cols=slice(None)):
        at = chip(step)
        return part[c][core * 4 + at, :, cols].astype(F32) + pair_in[c][at, :, cols].astype(F32)

    def do_sum(c):
        arrived(pair_in[c], t_recv.at[c, 0])
        if c in DIRECT:
            for n, step in enumerate((2, 1, -1)):
                acc[c][n] = chip_sum(c, step).astype(BF)
                send(acc[c].at[n], side_in[c].at[n], t_send.at[c], t_recv.at[c, 3], along_x(step))
            return
        cut = halves_of(c)
        acc[c][0] = chip_sum(c, 2).astype(BF)
        for n, direction in enumerate((1, -1)):
            send(acc[c].at[0, :, cut[n]], half_in[c].at[n], t_send.at[c], t_recv.at[c, 1 + n], along_x(direction))
        for n, direction in enumerate((1, -1)):
            ready = cut[1 - n]
            acc[c][1 + n, :, ready] = chip_sum(c, direction, ready).astype(BF)
            send(
                acc[c].at[1 + n, :, ready], side_in[c].at[n, :, ready],
                t_send.at[c], t_recv.at[c, 3], along_x(direction),
            )

    def do_on(c):
        cut = halves_of(c)
        for n, direction in enumerate((1, -1)):
            arrived(half_in[c].at[n], t_recv.at[c, 1 + n])
            acc[c][1 + n, :, cut[n]] = (chip_sum(c, direction, cut[n]) + half_in[c][n].astype(F32)).astype(BF)
            send(
                acc[c].at[1 + n, :, cut[n]], side_in[c].at[n, :, cut[n]],
                t_send.at[c], t_recv.at[c, 3], along_x(direction),
            )

    def do_done(c):
        cols = [carried[:, pl.ds(pl.multiple_of(unit(c, k) * 256, 256), 256)] for k in range(len(CHUNKS[c]))]
        mine = chip_sum(c, 0) + jnp.concatenate(cols, axis=1).astype(F32)
        arrived(side_in[c], t_recv.at[c, 3])
        for n in range(3 if c in DIRECT else 2):
            mine += side_in[c][n].astype(F32)
        final[c][tp] = mine.astype(BF)
        ref = final[c].at[tp]
        for n, step in enumerate((1, -1, 2) if c in DIRECT else (1, -1)):
            send(ref, ref, t_send.at[c], t_recv.at[c, 4 + n], along_x(step))
        send(ref, ref, t_send.at[c], t_recv.at[c, 8], partner)

    def do_pass(c):
        for n, step in enumerate((1, -1, 2) if c in DIRECT else (1, -1)):
            ref = final[c].at[along_x(-step)[1]]
            arrived(ref, t_recv.at[c, 4 + n])
            if c not in DIRECT:
                piece = ref.at[:, halves_of(c)[n]]
                send(piece, piece, t_send.at[c], t_recv.at[c, 6 + n], along_x(step))
            send(ref, ref, t_send.at[c], t_recv.at[c, 8], partner)

    def do_last(c):
        for n in range(2):
            piece = final[c].at[along_x(2)[1], :, halves_of(c)[n]]
            arrived(piece, t_recv.at[c, 6 + n])
            send(piece, piece, t_send.at[c], t_recv.at[c, 8], partner)

    def do_out(c):
        arrived(final[c].at[pl.ds(0, 4)], t_recv.at[c, 8])
        for k in range(len(CHUNKS[c])):
            cols = pl.ds(pl.multiple_of(unit(c, k) * 256, 256), 256)
            out[:, :, cols] = final[c][:, :, pl.ds(k * 256, 256)]

    def do_clean():
        for n in range(4):
            left(bufs[n].at[pl.ds(0, 63)], w_send.at[n])
        left(gains.at[pl.ds(0, 7)], m_send.at[0])
        left(ymsg.at[pl.ds(0, 7)], m_send.at[1])
        left(zmsg.at[pl.ds(0, 7)], m_send.at[2])
        left(act_out.at[pl.ds(0, 7)], m_send.at[3])
        left(mats.at[pl.ds(0, 7)], ag_send.at[0])
        left(normed.at[pl.ds(0, 7)], ag_send.at[1])

    do = {
        "ywait": do_ywait, "zwait": do_zwait, "readout": do_readout, "act": do_act, "proj": do_proj, "up": do_up,
        "clean": do_clean,
        "mats0": lambda: gather_middle(mats, 0, (0,)), "mats1": lambda: gather_middle(mats, 0, (1,)),
        "mats2": lambda: gather_end(mats, 0),
        "rows0": lambda: gather_middle(normed, 1, (0,)), "rows1": lambda: gather_middle(normed, 1, (1,)),
        "rows2": lambda: gather_end(normed, 1),
    }
    by_chunk = {
        "product": do_product, "sum": do_sum, "on": do_on, "done": do_done, "pass": do_pass, "last": do_last,
        "out": do_out,
    }
    started = False
    for kind, what in plan()[0]:
        if kind == "wait" and not started:
            started = True
            start_rest()
        if kind == "send":
            copy_send(what)
        elif kind == "wait":
            copy_wait(what)
        else:
            if what in do:
                do[what]()
            else:
                by_chunk[what[:-1]](int(what[-1]))
    for c, chunk in enumerate(CHUNKS):
        left(part[c], t_send.at[c])


def step(*args):
    args = list(args)
    for n in (10, 11, 13):
        args[n] = args[n].reshape(1, -1)
    args[4] = args[4].T
    for n in (6, 7):
        args[n] = jnp.swapaxes(args[n], 2, 3)
    args = [pltpu.with_memory_space_constraint(a, pltpu.HBM) for a in args]
    vmem, hbm = pl.BlockSpec(memory_space=pltpu.VMEM), pl.BlockSpec(memory_space=pltpu.HBM)
    dma = pltpu.SemaphoreType.DMA
    scratch = [
        *[pltpu.VMEM((64, 32, 512), BF)] * 4,
        pltpu.VMEM((8, 128, 2048), BF),
        pltpu.VMEM((8, 48, 2048), BF),
        pltpu.VMEM((48, 2048), BF),
        pltpu.VMEM((48, 2048), BF),
        *[pltpu.VMEM((384, STATES), F32)] * 3,
        *[pltpu.VMEM((8, 4, STATES), F32)] * 2,
        pltpu.VMEM((8, 1, 128), F32),
        pltpu.VMEM((8, 48, 128), BF),
        pltpu.VMEM((8, 48, 128), BF),
        pltpu.VMEM((384, 1024), BF),
        dma((6,)), dma((4,)), dma((4, 4)), dma((4, 32)), dma((4,)), dma((4,)),
        dma((2,)), dma((2, 7)), dma((4,)), dma((4, 9)), dma((8,)),
    ]
    for c, chunk in enumerate(CHUNKS):
        width = 256 * len(chunk)
        final = c in DIRECT
        scratch += [
            pltpu.VMEM((14, 48, width), BF),
            pltpu.VMEM((4, 48, width), BF),
            pltpu.VMEM((3, 48, width), BF),
            pltpu.VMEM((2, 48, width // 2), BF),
            pltpu.VMEM((3 if final else 2, 48, width), BF),
            pltpu.VMEM((8, 48, width), BF),
        ]
    whole = pl.pallas_call(
        kernel,
        out_shape=jax.ShapeDtypeStruct((8, 48, 2048), BF),
        in_specs=[hbm if n in (0, 12, 14, 15) else vmem for n in range(16)],
        out_specs=vmem,
        scratch_shapes=scratch,
        compiler_params=pltpu.CompilerParams(
            collective_id=0, has_side_effects=True, vmem_limit_bytes=48 * 1024 * 1024
        ),
    )(*args)
    return whole.reshape(384, 2048)


def solution(mesh):
    return jax.shard_map(
        step,
        mesh=mesh,
        in_specs=(
            P("sp", None),
            P("sp", "tp"),
            P(None, "tp", None),
            P(None, "tp", None),
            P("tp", None),
            P("tp", None, "sp"),
            P(None, "tp", None, None),
            P(None, "tp", None, None),
            P(None, "tp", None, None),
            P(None, "tp", None, None),
            P("tp"),
            P("tp"),
            P("tp", None),
            P(),
            P("sp", "tp"),
            P("sp", "tp"),
        ),
        out_specs=P("sp", None),
        check_vma=False,
    )
```

```python
import jax
import jax.numpy as jnp
from jax import lax
from jax.experimental import pallas as pl
from jax.experimental.pallas import tpu as pltpu
from jax.sharding import PartitionSpec as P

MESH = pl.DeviceIdType.MESH
BF, F32 = jnp.bfloat16, jnp.float32
EPS = 1e-06
NT = (((1,), (1,)), ((), ()))
STATES = 384
STEPS, LANES = 48, 8


def iota(shape, dim):
    return lax.broadcasted_iota(jnp.int32, shape, dim)


def one_row(values):
    rows, width = values.shape
    tiled = jnp.concatenate([values] * rows, axis=1)
    keep = iota(tiled.shape, 0) == iota(tiled.shape, 1) // width
    return jnp.sum(jnp.where(keep, tiled, 0.0), axis=0, keepdims=True)


def spread(line, width):
    keep = iota((4, 4), 0) == iota((4, 4), 1)
    column = jnp.sum(jnp.where(keep, jnp.broadcast_to(line, (4, 4)), 0.0), axis=1, keepdims=True)
    shape = (4, 4 * width)
    keep = iota(shape, 0) == iota(shape, 1) // width
    return jnp.sum(jnp.where(keep, jnp.broadcast_to(column, shape), 0.0), axis=0, keepdims=True)


def expm1_small(x):
    total = jnp.ones_like(x)
    for order in range(9, 1, -1):
        total = 1.0 + total * x * (1.0 / order)
    return total * x


def times(a, b):
    return a[0] * b[0] - a[1] * b[1], a[0] * b[1] + a[1] * b[0]


def discretize(wide_poles, narrow_poles, log_step):
    real = jnp.concatenate([one_row(wide_poles[0]), one_row(narrow_poles[0])], axis=1)
    imag = jnp.concatenate([one_row(wide_poles[1]), one_row(narrow_poles[1])], axis=1)
    steps = log_step[...]
    step = jnp.exp(jnp.concatenate([spread(steps[:1], 64), spread(steps[1:], 32)], axis=1))
    growth, angle = real * step, imag * step
    size, sine, cosine = jnp.exp(growth), jnp.sin(angle), jnp.cos(angle)
    half = jnp.sin(0.5 * angle)
    rise_real = expm1_small(growth) * cosine - 2.0 * half * half
    rise_imag = size * sine
    bottom = real * real + imag * imag
    coef_real = (rise_real * real + rise_imag * imag) / bottom
    coef_imag = (rise_imag * real - rise_real * imag) / bottom
    return (size * cosine, size * sine), (coef_real, coef_imag)


def blocks(first, second):
    out = []
    for part in range(2):
        halves = []
        for kind, (ref, width) in enumerate(((first, 64), (second, 32))):
            flat = ref[part].reshape(64, width)
            row, col = iota((128, 64), 0), iota((128, 64), 1)
            pick = ((row // 32 == col // 16) & (row % 16 == col % 16)).astype(BF)
            rows = jnp.dot(pick, flat, preferred_element_type=F32).astype(BF)
            repeat = (iota((width, 4 * width), 1) % width == iota((width, 4 * width), 0)).astype(BF)
            tiled = jnp.dot(rows, repeat, preferred_element_type=F32)
            row, col = iota(tiled.shape, 0), iota(tiled.shape, 1)
            keep = (row // 32 == col // width) & ((row // 16) % 2 == kind)
            halves.append(jnp.where(keep, tiled, 0.0))
        out.append(jnp.concatenate(halves, axis=1))
    return out


def order():
    row, col = iota((384, 384), 0), iota((384, 384), 1)
    return (col == (row % LANES) * STEPS + row // LANES).astype(BF)


def back_order():
    row, col = iota((384, 384), 0), iota((384, 384), 1)
    return (row == (col % LANES) * STEPS + col // LANES).astype(BF)


def decay_rows(forget, pick):
    rows = jnp.concatenate([forget[p] for p in range(4)], axis=0)
    high = rows.astype(BF)
    rest = rows - high.astype(F32)
    middle = rest.astype(BF)
    low = (rest - middle.astype(F32)).astype(BF)
    parts = jnp.concatenate([high.astype(F32), middle.astype(F32), low.astype(F32)], axis=0).astype(BF)
    turned = lax.dot_general(pick, parts, NT, preferred_element_type=F32).astype(BF)
    row, col = iota((24, STATES), 0), iota((24, STATES), 1)
    group = jnp.where(col < 256, 2 * (col // 64), 2 * ((col - 256) // 32) + 1)
    place = (row % 8 == group).astype(BF)
    return jnp.exp(-jnp.dot(turned, place, preferred_element_type=F32))


def chain(first, ends, decay, run_base):
    now, starts = first, []
    for run in range(LANES):
        starts.append(now)
        part = slice(run, run + 1)
        grown = times(run_base, now)
        now = (
            decay[part] * grown[0] + ends[0][part],
            decay[part] * grown[1] + ends[1][part],
        )
    return [jnp.concatenate([s[i] for s in starts], axis=0) for i in range(2)], now


OFFSETS = (0, -1, 1, -2, 2, -3, 3, 4)
GROUPS = ((0,), (1, 2), (3, 4), (5, 6), (7,))
RIGHTWARD = (0, 1, 3, 5)
CHUNKS = ((0, 1, 2), (3, 4), (5, 6), (7,))
DIRECT = (2, 3)
COPY, DELAY, ISSUE, AHEAD, FILL, LATE = 0.703, 2.6, 0.03, 1.8, 1.8, 0.6
DUE, UP_DUE = (32.0, 36.0, 42.0, 46.0), 15.0


def chunk_of(s):
    return [n for n, chunk in enumerate(CHUNKS) if GROUPS[s][0] in chunk][0]


def slack(op):
    kind, n, s, hop = op
    step = DELAY + COPY
    if kind == "first":
        return (0.0 if n < 2 else 8.0) + hop
    if n < 2:
        return UP_DUE - (4 - hop) * step
    if n == 3:
        return DUE[chunk_of(s)] - (4 - hop) * step
    return min(DUE[h - 1] - (h - hop) * step for h in range(hop, 5))


def waits_of(n, chunk=None):
    ops = []
    if chunk is None or chunk == 0:
        ops += [("first", n, 0, hop) for hop in range(1, 5)]
    for s in range(len(GROUPS)):
        for hop in range(1, 5):
            mine = chunk is None or (hop == chunk + 1 if n == 2 else chunk_of(s) == chunk)
            if mine:
                ops.append(("line", n, s, hop))
    return set(ops)


def steps_of():
    ups = waits_of(0) | waits_of(1)
    steps = {
        "local": ((), 0.0, 1.8, set()),
        "ywait": (("local",), 6.0, 0.1, set()),
        "zwait": (("ywait",), 8.0, 0.1, set()),
        "readout": (("zwait",), 0.0, 1.3, set()),
        "mats0": (("local",), 8.0, 0.05, set()),
        "mats1": (("mats0",), 5.6, 0.05, set()),
        "act": (("readout", "mats1"), 5.5, 0.2, set()),
        "mats2": (("mats1",), 5.0, 0.05, set()),
        "proj": (("act", "mats2"), 1.3, 1.0, set()),
        "rows0": (("proj",), 4.3, 0.05, set()),
        "rows1": (("rows0",), 2.1, 0.05, set()),
        "rows2": (("rows1",), 2.1, 0.05, set()),
        "up": (("rows2",), 1.3, 1.8, ups),
    }
    for c, chunk in enumerate(CHUNKS):
        width = len(chunk)
        needs = waits_of(2, c) | waits_of(3, c)
        steps[f"product{c}"] = (("up",) if c == 0 else ("up", f"product{c - 1}"), 0.0, 0.35 * width, needs)
        steps[f"sum{c}"] = ((f"product{c}",), 1.3 + 0.2 * width, 0.1, set())
        final = c in DIRECT
        if not final:
            steps[f"on{c}"] = ((f"sum{c}",), 2.4 + 0.5 * width, 0.1, set())
        steps[f"done{c}"] = ((f"sum{c}" if final else f"on{c}",), (3.2 + 1.0 * width) if final else 2.8 + 0.5 * width, 0.1, set())
        steps[f"pass{c}"] = ((f"done{c}",), 3.2 + 1.0 * width if final else 2.8 + 0.5 * width, 0.05, set())
        if not final:
            steps[f"last{c}"] = ((f"pass{c}",), 2.4 + 0.3 * width, 0.05, set())
        steps[f"out{c}"] = ((f"pass{c}" if final else f"last{c}",), 1.2, 0.05, set())
    steps["clean"] = ((f"product{len(CHUNKS) - 1}",), 0.1, 0.2, set())
    return steps


def plan():
    steps, order = steps_of(), []
    free, ready, coming = [LATE, LATE], [set(), set()], []
    ended, seen, now = {}, set(), 0.0

    def link(op):
        return (op[1] + (op[0] == "line")) % 2

    def offer(op):
        ready[link(op)].add(op)

    for n in range(4):
        offer(("first", n, 0, 1))
        offer(("line", n, 0, 1))
    while steps or coming or ready[0] or ready[1]:
        for side in range(2):
            ahead = 0.0
            for name, (before, after, own, needs) in steps.items():
                if own > 0.9 and all(b in ended for b in before) and needs <= seen:
                    if max([ended[b] for b in before], default=0.0) + after < now + 0.3:
                        ahead = own
            while ready[side]:
                op = min(ready[side], key=lambda o: (slack(o), o))
                if free[side] - now >= (1.0 + LATE if "local" not in ended else ahead + (AHEAD if op[1] < 2 else FILL)):
                    break
                ready[side].remove(op)
                order.append(("send", op))
                both = 1.0 if op[3] < 4 else 0.5
                both *= 1 if op[0] == "first" else len(GROUPS[op[2]])
                free[side] = max(free[side], now) + COPY * both
                coming.append((free[side] + DELAY, op))
                now += ISSUE
        due = min(coming, default=None)
        able = [
            (max([ended[b] for b in before], default=0.0) + after, name)
            for name, (before, after, _, needs) in steps.items()
            if all(b in ended for b in before) and needs <= seen
        ]
        step = min(able, default=None)
        if due and due[0] <= now or (due and (step is None or due[0] < step[0])):
            now = max(now, due[0]) + ISSUE
            coming.remove(due)
            op = due[1]
            seen.add(op)
            order.append(("wait", op))
            kind, n, s, hop = op
            if hop < 4:
                offer((kind, n, s, hop + 1))
            if kind == "first":
                offer(("line", n, hop, 1))
        elif step:
            wake = [free[side] - FILL * 0.5 for side in range(2) if ready[side]]
            if wake and min(wake) < step[0] and min(wake) > now:
                now = min(wake)
                continue
            now = max(now, step[0]) + steps[step[1]][2]
            ended[step[1]] = now
            order.append(("step", step[1]))
            if step[1] in ("local", "ywait"):
                side = int(step[1] == "ywait")
                free[side] = max(free[side], now) + 1.0
            del steps[step[1]]
        else:
            now = max(now, min(free[side] for side in range(2) if ready[side]) - FILL * 0.5)
    return order, ended, now


def kernel(
    hidden_in, drive_in, wide_poles_in, narrow_poles_in, log_step_in, forget_in, wide_input_in, narrow_input_in,
    wide_output_in, narrow_output_in, skip_in, mix_gain_in, out_weight, mlp_gain_in, up_weight, down_weight,
    out,
    drive, wide_poles, narrow_poles, log_step, forget, wide_input, narrow_input,
    wide_output, narrow_output, skip, mix_gain, mlp_gain,
    up_a, up_b, dn_a, dn_b, mats, normed, own_in, carried,
    push_r, push_i, decay, ymsg, zmsg, gains, act_out, act_in, squared,
    loc_sem, w_send, s1_recv, s2_recv, m_send, m_recv, ag_send, ag_recv, t_send, t_recv,
    *pieces,
):
    part, pair_in, acc, half_in, side_in, final = (pieces[n :: 6] for n in range(6))
    sp, tp = lax.axis_index("sp"), lax.axis_index("tp")
    y, z, x, core = sp % 8, sp // 8, tp // 2, tp % 2

    def along_y(step):
        return z * 8 + (y + step + 8) % 8, tp

    def along_z(step):
        return ((z + step + 8) % 8) * 8 + y, tp

    def group(step):
        return sp, (tp + step) % 8

    def along_x(step):
        return sp, ((x + step + 4) % 4) * 2 + core

    partner = (sp, 2 * x + 1 - core)

    def send(src, dst, send_sem, recv_sem, to):
        pltpu.make_async_remote_copy(
            src_ref=src, dst_ref=dst, send_sem=send_sem, recv_sem=recv_sem, device_id=to, device_id_type=MESH
        ).start()

    def held(ref, sem):
        return pltpu.make_async_remote_copy(
            src_ref=ref, dst_ref=ref, send_sem=sem, recv_sem=sem, device_id=partner, device_id_type=MESH
        )

    def arrived(dst, recv_sem):
        held(dst, recv_sem).wait_recv()

    def left(src, send_sem):
        held(src, send_sem).wait_send()

    barrier = pltpu.get_barrier_semaphore()
    for step in range(1, 8):
        for to in (along_y(step), along_z(step), group(step)):
            pl.semaphore_signal(barrier, inc=1, device_id=to, device_id_type=MESH)
    bufs = (up_a, up_b, dn_a, dn_b)

    def where_of(n):
        return (y, z, along_y, along_z) if n % 2 == 0 else (z, y, along_z, along_y)

    def shard(n, first, second):
        return bufs[n].at[second * 8 + first]

    def mod8(v):
        return (v + 8) % 8

    local = []
    for n, weight in enumerate((up_weight, up_weight, down_weight, down_weight)):
        at, line, _, _ = where_of(n)
        local.append(
            pltpu.make_async_copy(weight.at[:, pl.ds((n % 2) * 512, 512)], shard(n, at, line), loc_sem.at[n])
        )
    local.append(pltpu.make_async_copy(out_weight, mats.at[tp], loc_sem.at[4]))
    local.append(pltpu.make_async_copy(hidden_in.at[pl.ds(pl.multiple_of(tp * 48, 16), 48)], own_in, loc_sem.at[5]))
    small = (
        (drive_in, drive), (wide_poles_in, wide_poles), (narrow_poles_in, narrow_poles), (log_step_in, log_step),
        (forget_in, forget), (wide_input_in, wide_input), (narrow_input_in, narrow_input),
        (wide_output_in, wide_output), (narrow_output_in, narrow_output), (skip_in, skip),
        (mix_gain_in, mix_gain), (mlp_gain_in, mlp_gain),
    )
    fetched = [pltpu.make_async_copy(src, dst, loc_sem.at[6 + n]) for n, (src, dst) in enumerate(small)]
    for copy in local[:4] + fetched + local[4:]:
        copy.start()
    def first_send(n, hop):
        at, line, go, _ = where_of(n)
        for direction in (1, -1) if hop < 4 else (1,):
            ref = shard(n, mod8(at - direction * (hop - 1)), line)
            send(ref, ref, w_send.at[n], s1_recv.at[n, hop - 1], go(direction))

    def line_send(n, s, hop):
        at, line, _, go = where_of(n)
        for k in GROUPS[s]:
            for direction in (1, -1):
                if hop < 4 or (k in RIGHTWARD) == (direction > 0):
                    ref = shard(n, mod8(at + OFFSETS[k]), mod8(line - direction * (hop - 1)))
                    send(ref, ref, w_send.at[n], s2_recv.at[n, 4 * s + hop - 1], go(direction))

    def copy_send(op):
        kind, n, s, hop = op
        if kind == "first":
            first_send(n, hop)
        else:
            line_send(n, s, hop)

    def copy_wait(op):
        kind, n, s, hop = op
        sem = s1_recv.at[n, hop - 1] if kind == "first" else s2_recv.at[n, 4 * s + hop - 1]
        count = (2 if hop < 4 else 1) * (1 if kind == "first" else len(GROUPS[s]))
        arrived(bufs[n].at[pl.ds(0, count)], sem)

    halves = (pl.ds(0, 1024), pl.ds(1024, 1024))

    def gather_start(buf, g):
        ref = buf.at[tp]
        for turn in range(2):
            for n, direction in enumerate((1, -1)):
                half = (n + turn) % 2
                piece = ref.at[:, halves[half]]
                send(piece, piece, ag_send.at[g], ag_recv.at[g, 2 * n + turn], along_x(direction))
        send(ref, ref, ag_send.at[g], ag_recv.at[g, 6], partner)

    def gather_middle(buf, g, turns=(0, 1)):
        for turn in turns:
            for n, direction in enumerate((1, -1)):
                half = (n + turn) % 2
                piece = buf.at[along_x(-direction)[1], :, halves[half]]
                arrived(piece, ag_recv.at[g, 2 * n + turn])
                if turn == 0:
                    send(piece, piece, ag_send.at[g], ag_recv.at[g, 4 + n], along_x(direction))
                send(piece, piece, ag_send.at[g], ag_recv.at[g, 6], partner)

    def gather_end(buf, g):
        far = buf.at[along_x(2)[1]]
        for n in range(2):
            piece = far.at[:, halves[n]]
            arrived(piece, ag_recv.at[g, 4 + n])
            send(piece, piece, ag_send.at[g], ag_recv.at[g, 6], partner)

    def gather_partner(buf, g):
        arrived(buf.at[pl.ds(0, 4)], ag_recv.at[g, 6])

    def message(buf, at, state, fade):
        buf[at] = jnp.concatenate([state[0], state[1], fade, fade], axis=0)

    for copy in local[:4]:
        copy.wait()
    pl.semaphore_wait(barrier, 21)
    held_values = {}

    def do_local():
        for copy in fetched + local[4:]:
            copy.wait()
        pick = order()
        decay[...] = decay_rows(forget, pick)
        drive_now = jnp.dot(pick, drive[...], preferred_element_type=F32).astype(BF)
        base, coef = discretize(wide_poles, narrow_poles, log_step)
        weights = [b.astype(BF) for b in blocks(wide_input, narrow_input)]
        pushed = times(coef, [jnp.dot(drive_now, w, preferred_element_type=F32) for w in weights])
        push_r[...] = pushed[0]
        push_i[...] = pushed[1]
        wide_base = [jnp.broadcast_to(b, (LANES, STATES)) for b in base]

        def scan_step(step, state):
            rows = pl.ds(pl.multiple_of(step * LANES, LANES), LANES)
            fade = decay[rows]
            grown = times(wide_base, state[:2])
            new = fade * grown[0] + push_r[rows], fade * grown[1] + push_i[rows], fade * state[2]
            push_r[rows], push_i[rows], decay[rows] = new
            return new

        zero = jnp.zeros((LANES, STATES), F32)
        end_r, end_i, total = lax.fori_loop(0, STEPS, scan_step, (zero, zero, zero + 1.0), unroll=4)
        powers = [base]
        for _ in range(5):
            powers.append(times(powers[-1], powers[-1]))
        run_base = times(powers[5], powers[4])
        _, last = chain((zero[:1], zero[:1]), (end_r, end_i), total, run_base)
        fade_all = total[:1]
        for run in range(1, LANES):
            fade_all = fade_all * total[run : run + 1]
        device_base = run_base
        for _ in range(3):
            device_base = times(device_base, device_base)
        line_base = device_base
        for _ in range(3):
            line_base = times(line_base, line_base)


        message(ymsg, y, last, fade_all)
        for step in range(1, 8):
            send(ymsg.at[y], ymsg.at[y], m_send.at[1], m_recv.at[1], along_y(step))
        gather_start(mats, 0)
        gains[tp] = mix_gain[...]
        for step in range(1, 8):
            send(mix_gain, gains.at[tp], m_send.at[0], m_recv.at[0], group(step))
        held_values["local"] = zero, wide_base, end_r, end_i, total, run_base, device_base, line_base, drive_now

    def do_ywait():
        arrived(ymsg.at[pl.ds(0, 7)], m_recv.at[1])
        zero, _, _, _, _, _, device_base, _, _ = held_values["local"]
        zrow, onerow = zero[:1], zero[:1] + 1.0
        whole, before = (zrow, zrow), (zrow, zrow)
        whole_fade, before_fade, before_base = onerow, onerow, (onerow, zrow)
        for k in range(8):
            got = ymsg[k]
            fade = got[2:3]
            grown = times(device_base, whole)
            new = fade * grown[0] + got[0:1], fade * grown[1] + got[1:2]
            new_fade = whole_fade * fade
            new_base = times(before_base, device_base)
            earlier = k < y
            before = [jnp.where(earlier, n, o) for n, o in zip(new, before)]
            before_fade = jnp.where(earlier, new_fade, before_fade)
            before_base = [jnp.where(earlier, n, o) for n, o in zip(new_base, before_base)]
            whole, whole_fade = new, new_fade

        message(zmsg, z, whole, whole_fade)
        for step in range(1, 8):
            send(zmsg.at[z], zmsg.at[z], m_send.at[2], m_recv.at[2], along_z(step))
        held_values["before"] = before, before_fade, before_base

    def do_zwait():
        arrived(zmsg.at[pl.ds(0, 7)], m_recv.at[2])
        before, before_fade, before_base = held_values["before"]
        zero, _, _, _, _, _, _, line_base, _ = held_values["local"]
        zrow = zero[:1]
        enter = (zrow, zrow)
        for k in range(8):
            got = zmsg[k]
            grown = times(line_base, enter)
            new = got[2:3] * grown[0] + got[0:1], got[2:3] * grown[1] + got[1:2]
            enter = [jnp.where(k < z, n, o) for n, o in zip(new, enter)]
        grown = times(before_base, enter)
        enter = before_fade * grown[0] + before[0], before_fade * grown[1] + before[1]

        held_values["enter"] = enter

    def do_readout():
        enter = held_values["enter"]
        _, wide_base, end_r, end_i, total, run_base, _, _, drive_now = held_values["local"]
        starts, _ = chain(enter, (end_r, end_i), total, run_base)

        def fix_step(step, state):
            rows = pl.ds(pl.multiple_of(step * LANES, LANES), LANES)
            state = times(wide_base, state)
            push_r[rows] = push_r[rows] + decay[rows] * state[0]
            push_i[rows] = push_i[rows] + decay[rows] * state[1]
            return state

        lax.fori_loop(0, STEPS, fix_step, tuple(starts), unroll=4)
        real_block, imag_block = blocks(wide_output, narrow_output)
        response = lax.dot_general(push_r[...].astype(BF), real_block.astype(BF), NT, preferred_element_type=F32)
        response -= lax.dot_general(push_i[...].astype(BF), imag_block.astype(BF), NT, preferred_element_type=F32)
        response += skip[...] * drive_now.astype(F32)
        active = 0.5 * response * (1.0 + lax.erf(response * (0.5**0.5)))
        active = jnp.dot(back_order(), active.astype(BF), preferred_element_type=F32).astype(BF)

        act_out[...] = active.reshape(8, 48, 128)
        act_in[tp] = act_out[tp]
        for step in range(1, 8):
            to = group(step)
            send(act_out.at[to[1]], act_in.at[tp], m_send.at[3], m_recv.at[3], to)

    def do_act():
        arrived(gains.at[pl.ds(0, 7)], m_recv.at[0])
        arrived(act_in.at[pl.ds(0, 7)], m_recv.at[3])
        rows = jnp.concatenate([act_in[k] for k in range(8)], axis=1).astype(F32)
        gain = jnp.concatenate([gains[k] for k in range(8)], axis=1)
        power = jnp.sum(rows * rows, axis=1, keepdims=True) * (1.0 / 1024)
        held_values["mixed"] = (rows * lax.rsqrt(power + EPS) * gain).astype(BF)

    def do_proj():
        gather_partner(mats, 0)
        for n in range(8):
            cols = pl.ds(n * 256, 256)
            proj = jnp.dot(held_values["mixed"], mats[:, :, cols].reshape(1024, 256), preferred_element_type=F32)
            carried[:, cols] = (own_in[:, cols].astype(F32) + proj).astype(BF)
        values = carried[...].astype(F32)
        power = jnp.sum(values * values, axis=1, keepdims=True) * (1.0 / 2048)
        normed[tp] = (values * lax.rsqrt(power + EPS) * mlp_gain[...]).astype(BF)
        gather_start(normed, 1)

    def do_up():
        gather_partner(normed, 1)
        for n in range(4):
            cols = pl.ds((n % 2) * 256, 256)
            buf = bufs[n // 2]
            if n < 2:
                weight = buf[:, :, cols].reshape(2048, 256)
            else:
                weight = jnp.concatenate([buf[(s % 8) * 8 + s // 8, :, cols] for s in range(64)], axis=0)
            pre = jnp.dot(normed[...].reshape(384, 2048), weight, preferred_element_type=F32)
            pre = jnp.maximum(pre, 0.0)
            squared[:, pl.ds(n * 256, 256)] = (pre * pre).astype(BF)

    def chip(step):
        return (x + step + 4) % 4

    def halves_of(c):
        half = len(CHUNKS[c]) * 128
        return pl.ds(0, half), pl.ds(half, half)

    def unit(c, k):
        return mod8(z + OFFSETS[CHUNKS[c][k]])

    def do_product(c):
        for k in range(len(CHUNKS[c])):
            q = unit(c, k)
            first = dn_a[pl.ds(pl.multiple_of(q * 8, 8), 8)].reshape(256, 512)
            second = jnp.concatenate([dn_b[s * 8 + q] for s in range(8)], axis=0)
            piece = lax.dot_general(squared[:, :512], first, NT, preferred_element_type=F32)
            piece += lax.dot_general(squared[:, 512:], second, NT, preferred_element_type=F32)
            piece = piece.astype(BF)
            for b in range(8):
                part[c][(b % 2) * 4 + b // 2, :, pl.ds(k * 256, 256)] = piece[b * 48 : (b + 1) * 48]
        send(part[c].at[pl.ds((1 - core) * 4, 4)], pair_in[c], t_send.at[c], t_recv.at[c, 0], partner)

    def chip_sum(c, step, cols=slice(None)):
        at = chip(step)
        return part[c][core * 4 + at, :, cols].astype(F32) + pair_in[c][at, :, cols].astype(F32)

    def do_sum(c):
        arrived(pair_in[c], t_recv.at[c, 0])
        if c in DIRECT:
            for n, step in enumerate((2, 1, -1)):
                acc[c][n] = chip_sum(c, step).astype(BF)
                send(acc[c].at[n], side_in[c].at[n], t_send.at[c], t_recv.at[c, 3], along_x(step))
            return
        cut = halves_of(c)
        acc[c][0] = chip_sum(c, 2).astype(BF)
        for n, direction in enumerate((1, -1)):
            send(acc[c].at[0, :, cut[n]], half_in[c].at[n], t_send.at[c], t_recv.at[c, 1 + n], along_x(direction))
        for n, direction in enumerate((1, -1)):
            ready = cut[1 - n]
            acc[c][1 + n, :, ready] = chip_sum(c, direction, ready).astype(BF)
            send(
                acc[c].at[1 + n, :, ready], side_in[c].at[n, :, ready],
                t_send.at[c], t_recv.at[c, 3], along_x(direction),
            )

    def do_on(c):
        cut = halves_of(c)
        for n, direction in enumerate((1, -1)):
            arrived(half_in[c].at[n], t_recv.at[c, 1 + n])
            acc[c][1 + n, :, cut[n]] = (chip_sum(c, direction, cut[n]) + half_in[c][n].astype(F32)).astype(BF)
            send(
                acc[c].at[1 + n, :, cut[n]], side_in[c].at[n, :, cut[n]],
                t_send.at[c], t_recv.at[c, 3], along_x(direction),
            )

    def do_done(c):
        cols = [carried[:, pl.ds(pl.multiple_of(unit(c, k) * 256, 256), 256)] for k in range(len(CHUNKS[c]))]
        mine = chip_sum(c, 0) + jnp.concatenate(cols, axis=1).astype(F32)
        arrived(side_in[c], t_recv.at[c, 3])
        for n in range(3 if c in DIRECT else 2):
            mine += side_in[c][n].astype(F32)
        final[c][tp] = mine.astype(BF)
        ref = final[c].at[tp]
        for n, step in enumerate((1, -1, 2) if c in DIRECT else (1, -1)):
            send(ref, ref, t_send.at[c], t_recv.at[c, 4 + n], along_x(step))
        send(ref, ref, t_send.at[c], t_recv.at[c, 8], partner)

    def do_pass(c):
        for n, step in enumerate((1, -1, 2) if c in DIRECT else (1, -1)):
            ref = final[c].at[along_x(-step)[1]]
            arrived(ref, t_recv.at[c, 4 + n])
            if c not in DIRECT:
                piece = ref.at[:, halves_of(c)[n]]
                send(piece, piece, t_send.at[c], t_recv.at[c, 6 + n], along_x(step))
            send(ref, ref, t_send.at[c], t_recv.at[c, 8], partner)

    def do_last(c):
        for n in range(2):
            piece = final[c].at[along_x(2)[1], :, halves_of(c)[n]]
            arrived(piece, t_recv.at[c, 6 + n])
            send(piece, piece, t_send.at[c], t_recv.at[c, 8], partner)

    def do_out(c):
        arrived(final[c].at[pl.ds(0, 4)], t_recv.at[c, 8])
        for k in range(len(CHUNKS[c])):
            cols = pl.ds(pl.multiple_of(unit(c, k) * 256, 256), 256)
            out[:, :, cols] = final[c][:, :, pl.ds(k * 256, 256)]

    def do_clean():
        for n in range(4):
            left(bufs[n].at[pl.ds(0, 63)], w_send.at[n])
        left(gains.at[pl.ds(0, 7)], m_send.at[0])
        left(ymsg.at[pl.ds(0, 7)], m_send.at[1])
        left(zmsg.at[pl.ds(0, 7)], m_send.at[2])
        left(act_out.at[pl.ds(0, 7)], m_send.at[3])
        left(mats.at[pl.ds(0, 7)], ag_send.at[0])
        left(normed.at[pl.ds(0, 7)], ag_send.at[1])

    do = {
        "local": do_local, "ywait": do_ywait, "zwait": do_zwait, "readout": do_readout, "act": do_act, "proj": do_proj, "up": do_up,
        "clean": do_clean,
        "mats0": lambda: gather_middle(mats, 0, (0,)), "mats1": lambda: gather_middle(mats, 0, (1,)),
        "mats2": lambda: gather_end(mats, 0),
        "rows0": lambda: gather_middle(normed, 1, (0,)), "rows1": lambda: gather_middle(normed, 1, (1,)),
        "rows2": lambda: gather_end(normed, 1),
    }
    by_chunk = {
        "product": do_product, "sum": do_sum, "on": do_on, "done": do_done, "pass": do_pass, "last": do_last,
        "out": do_out,
    }
    for kind, what in plan()[0]:
        if kind == "send":
            copy_send(what)
        elif kind == "wait":
            copy_wait(what)
        else:
            if what in do:
                do[what]()
            else:
                by_chunk[what[:-1]](int(what[-1]))
    for c in range(len(CHUNKS)):
        left(part[c], t_send.at[c])


def step(*args):
    args = list(args)
    for n in (10, 11, 13):
        args[n] = args[n].reshape(1, -1)
    args[4] = args[4].T
    for n in (6, 7):
        args[n] = jnp.swapaxes(args[n], 2, 3)
    args = [pltpu.with_memory_space_constraint(a, pltpu.HBM) for a in args]
    vmem, hbm = pl.BlockSpec(memory_space=pltpu.VMEM), pl.BlockSpec(memory_space=pltpu.HBM)
    dma = pltpu.SemaphoreType.DMA
    scratch = [
        *[pltpu.VMEM(a.shape, a.dtype) for n, a in enumerate(args) if n not in (0, 12, 14, 15)],
        *[pltpu.VMEM((64, 32, 512), BF)] * 4,
        pltpu.VMEM((8, 128, 2048), BF),
        pltpu.VMEM((8, 48, 2048), BF),
        pltpu.VMEM((48, 2048), BF),
        pltpu.VMEM((48, 2048), BF),
        *[pltpu.VMEM((384, STATES), F32)] * 3,
        *[pltpu.VMEM((8, 4, STATES), F32)] * 2,
        pltpu.VMEM((8, 1, 128), F32),
        pltpu.VMEM((8, 48, 128), BF),
        pltpu.VMEM((8, 48, 128), BF),
        pltpu.VMEM((384, 1024), BF),
        dma((18,)), dma((4,)), dma((4, 4)), dma((4, 20)), dma((4,)), dma((4,)),
        dma((2,)), dma((2, 7)), dma((4,)), dma((4, 9)),
    ]
    for c, chunk in enumerate(CHUNKS):
        width = 256 * len(chunk)
        final = c in DIRECT
        scratch += [
            pltpu.VMEM((14, 48, width), BF),
            pltpu.VMEM((4, 48, width), BF),
            pltpu.VMEM((3, 48, width), BF),
            pltpu.VMEM((2, 48, width // 2), BF),
            pltpu.VMEM((3 if final else 2, 48, width), BF),
            pltpu.VMEM((8, 48, width), BF),
        ]
    whole = pl.pallas_call(
        kernel,
        out_shape=jax.ShapeDtypeStruct((8, 48, 2048), BF),
        in_specs=[hbm] * 16,
        out_specs=vmem,
        scratch_shapes=scratch,
        compiler_params=pltpu.CompilerParams(
            collective_id=0, has_side_effects=True, vmem_limit_bytes=48 * 1024 * 1024
        ),
    )(*args)
    return whole.reshape(384, 2048)


def solution(mesh):
    return jax.shard_map(
        step,
        mesh=mesh,
        in_specs=(
            P("sp", None),
            P("sp", "tp"),
            P(None, "tp", None),
            P(None, "tp", None),
            P("tp", None),
            P("tp", None, "sp"),
            P(None, "tp", None, None),
            P(None, "tp", None, None),
            P(None, "tp", None, None),
            P(None, "tp", None, None),
            P("tp"),
            P("tp"),
            P("tp", None),
            P(),
            P("sp", "tp"),
            P("sp", "tp"),
        ),
        out_specs=P("sp", None),
        check_vma=False,
    )
```

```python
import jax
import jax.numpy as jnp
from jax import lax
from jax.experimental import pallas as pl
from jax.experimental.pallas import tpu as pltpu
from jax.sharding import PartitionSpec as P

MESH = pl.DeviceIdType.MESH
BF, F32 = jnp.bfloat16, jnp.float32
EPS = 1e-06
NT = (((1,), (1,)), ((), ()))
STATES = 384
STEPS, LANES = 48, 8


def iota(shape, dim):
    return lax.broadcasted_iota(jnp.int32, shape, dim)


def one_row(values):
    rows, width = values.shape
    tiled = jnp.concatenate([values] * rows, axis=1)
    keep = iota(tiled.shape, 0) == iota(tiled.shape, 1) // width
    return jnp.sum(jnp.where(keep, tiled, 0.0), axis=0, keepdims=True)


def spread(line, width):
    keep = iota((4, 4), 0) == iota((4, 4), 1)
    column = jnp.sum(jnp.where(keep, jnp.broadcast_to(line, (4, 4)), 0.0), axis=1, keepdims=True)
    shape = (4, 4 * width)
    keep = iota(shape, 0) == iota(shape, 1) // width
    return jnp.sum(jnp.where(keep, jnp.broadcast_to(column, shape), 0.0), axis=0, keepdims=True)


def expm1_small(x):
    total = jnp.ones_like(x)
    for order in range(9, 1, -1):
        total = 1.0 + total * x * (1.0 / order)
    return total * x


def times(a, b):
    return a[0] * b[0] - a[1] * b[1], a[0] * b[1] + a[1] * b[0]


def discretize(wide_poles, narrow_poles, log_step):
    real = jnp.concatenate([one_row(wide_poles[0]), one_row(narrow_poles[0])], axis=1)
    imag = jnp.concatenate([one_row(wide_poles[1]), one_row(narrow_poles[1])], axis=1)
    steps = log_step[...]
    step = jnp.exp(jnp.concatenate([spread(steps[:1], 64), spread(steps[1:], 32)], axis=1))
    growth, angle = real * step, imag * step
    size, sine, cosine = jnp.exp(growth), jnp.sin(angle), jnp.cos(angle)
    half = jnp.sin(0.5 * angle)
    rise_real = expm1_small(growth) * cosine - 2.0 * half * half
    rise_imag = size * sine
    bottom = real * real + imag * imag
    coef_real = (rise_real * real + rise_imag * imag) / bottom
    coef_imag = (rise_imag * real - rise_real * imag) / bottom
    return (size * cosine, size * sine), (coef_real, coef_imag)


def blocks(first, second):
    out = []
    for part in range(2):
        halves = []
        for kind, (ref, width) in enumerate(((first, 64), (second, 32))):
            flat = ref[part].reshape(64, width)
            row, col = iota((128, 64), 0), iota((128, 64), 1)
            pick = ((row // 32 == col // 16) & (row % 16 == col % 16)).astype(BF)
            rows = jnp.dot(pick, flat, preferred_element_type=F32).astype(BF)
            repeat = (iota((width, 4 * width), 1) % width == iota((width, 4 * width), 0)).astype(BF)
            tiled = jnp.dot(rows, repeat, preferred_element_type=F32)
            row, col = iota(tiled.shape, 0), iota(tiled.shape, 1)
            keep = (row // 32 == col // width) & ((row // 16) % 2 == kind)
            halves.append(jnp.where(keep, tiled, 0.0))
        out.append(jnp.concatenate(halves, axis=1))
    return out


def order():
    row, col = iota((384, 384), 0), iota((384, 384), 1)
    return (col == (row % LANES) * STEPS + row // LANES).astype(BF)


def back_order():
    row, col = iota((384, 384), 0), iota((384, 384), 1)
    return (row == (col % LANES) * STEPS + col // LANES).astype(BF)


def decay_rows(forget, pick):
    rows = jnp.concatenate([forget[p] for p in range(4)], axis=0)
    high = rows.astype(BF)
    rest = rows - high.astype(F32)
    middle = rest.astype(BF)
    low = (rest - middle.astype(F32)).astype(BF)
    parts = jnp.concatenate([high.astype(F32), middle.astype(F32), low.astype(F32)], axis=0).astype(BF)
    turned = lax.dot_general(pick, parts, NT, preferred_element_type=F32).astype(BF)
    row, col = iota((24, STATES), 0), iota((24, STATES), 1)
    group = jnp.where(col < 256, 2 * (col // 64), 2 * ((col - 256) // 32) + 1)
    place = (row % 8 == group).astype(BF)
    return jnp.exp(-jnp.dot(turned, place, preferred_element_type=F32))


def chain(first, ends, decay, run_base):
    now, starts = first, []
    for run in range(LANES):
        starts.append(now)
        part = slice(run, run + 1)
        grown = times(run_base, now)
        now = (
            decay[part] * grown[0] + ends[0][part],
            decay[part] * grown[1] + ends[1][part],
        )
    return [jnp.concatenate([s[i] for s in starts], axis=0) for i in range(2)], now


OFFSETS = (0, -1, 1, -2, 2, -3, 3, 4)
GROUPS = ((0,), (1, 2), (3, 4), (5, 6), (7,))
RIGHTWARD = (0, 1, 3, 5)
CHUNKS = ((0, 1, 2), (3, 4), (5, 6), (7,))
DIRECT = (0, 1, 2, 3)
COPY, DELAY, ISSUE, AHEAD, FILL, LATE = 0.703, 2.6, 0.03, 1.8, 1.8, 0.6
DUE, UP_DUE = (32.0, 36.0, 42.0, 46.0), 15.0


def chunk_of(s):
    return [n for n, chunk in enumerate(CHUNKS) if GROUPS[s][0] in chunk][0]


def slack(op):
    kind, n, s, hop = op
    step = DELAY + COPY
    if kind == "first":
        return (0.0 if n < 2 else 8.0) + hop
    if n < 2:
        return UP_DUE - (4 - hop) * step
    if n == 3:
        return DUE[chunk_of(s)] - (4 - hop) * step
    return min(DUE[h - 1] - (h - hop) * step for h in range(hop, 5))


def waits_of(n, chunk=None):
    ops = []
    if chunk is None or chunk == 0:
        ops += [("first", n, 0, hop) for hop in range(1, 5)]
    for s in range(len(GROUPS)):
        for hop in range(1, 5):
            mine = chunk is None or (hop == chunk + 1 if n == 2 else chunk_of(s) == chunk)
            if mine:
                ops.append(("line", n, s, hop))
    return set(ops)


def steps_of():
    ups = waits_of(0) | waits_of(1)
    steps = {
        "local": ((), 0.0, 1.8, set()),
        "ywait": (("local",), 6.0, 0.1, set()),
        "zwait": (("ywait",), 8.0, 0.1, set()),
        "readout": (("zwait",), 0.0, 1.3, set()),
        "mats0": (("local",), 8.0, 0.05, set()),
        "mats1": (("mats0",), 5.6, 0.05, set()),
        "act": (("readout", "mats1"), 5.5, 0.2, set()),
        "mats2": (("mats1",), 5.0, 0.05, set()),
        "proj": (("act", "mats2"), 1.3, 1.0, set()),
        "rows0": (("proj",), 4.3, 0.05, set()),
        "rows1": (("rows0",), 2.1, 0.05, set()),
        "rows2": (("rows1",), 2.1, 0.05, set()),
        "up": (("rows2",), 1.3, 1.8, ups),
    }
    for c, chunk in enumerate(CHUNKS):
        width = len(chunk)
        needs = waits_of(2, c) | waits_of(3, c)
        steps[f"product{c}"] = (("up",) if c == 0 else ("up", f"product{c - 1}"), 0.0, 0.35 * width, needs)
        steps[f"sum{c}"] = ((f"product{c}",), 1.3 + 0.2 * width, 0.1, set())
        final = c in DIRECT
        if not final:
            steps[f"on{c}"] = ((f"sum{c}",), 2.4 + 0.5 * width, 0.1, set())
        steps[f"done{c}"] = ((f"sum{c}" if final else f"on{c}",), (3.2 + 1.0 * width) if final else 2.8 + 0.5 * width, 0.1, set())
        steps[f"pass{c}"] = ((f"done{c}",), 3.2 + 1.0 * width if final else 2.8 + 0.5 * width, 0.05, set())
        if not final:
            steps[f"last{c}"] = ((f"pass{c}",), 2.4 + 0.3 * width, 0.05, set())
        steps[f"out{c}"] = ((f"pass{c}" if final else f"last{c}",), 1.2, 0.05, set())
    steps["clean"] = ((f"product{len(CHUNKS) - 1}",), 0.1, 0.2, set())
    return steps


def plan():
    steps, order = steps_of(), []
    free, ready, coming = [LATE, LATE], [set(), set()], []
    ended, seen, now = {}, set(), 0.0

    def link(op):
        return (op[1] + (op[0] == "line")) % 2

    def offer(op):
        ready[link(op)].add(op)

    for n in range(4):
        offer(("first", n, 0, 1))
        offer(("line", n, 0, 1))
    while steps or coming or ready[0] or ready[1]:
        for side in range(2):
            ahead = 0.0
            for name, (before, after, own, needs) in steps.items():
                if own > 0.9 and all(b in ended for b in before) and needs <= seen:
                    if max([ended[b] for b in before], default=0.0) + after < now + 0.3:
                        ahead = own
            while ready[side]:
                op = min(ready[side], key=lambda o: (slack(o), o))
                if free[side] - now >= (1.0 + LATE if "local" not in ended else ahead + (AHEAD if op[1] < 2 else FILL)):
                    break
                ready[side].remove(op)
                order.append(("send", op))
                both = 1.0 if op[3] < 4 else 0.5
                both *= 1 if op[0] == "first" else len(GROUPS[op[2]])
                free[side] = max(free[side], now) + COPY * both
                coming.append((free[side] + DELAY, op))
                now += ISSUE
        due = min(coming, default=None)
        able = [
            (max([ended[b] for b in before], default=0.0) + after, name)
            for name, (before, after, _, needs) in steps.items()
            if all(b in ended for b in before) and needs <= seen
        ]
        step = min(able, default=None)
        if due and due[0] <= now or (due and (step is None or due[0] < step[0])):
            now = max(now, due[0]) + ISSUE
            coming.remove(due)
            op = due[1]
            seen.add(op)
            order.append(("wait", op))
            kind, n, s, hop = op
            if hop < 4:
                offer((kind, n, s, hop + 1))
            if kind == "first":
                offer(("line", n, hop, 1))
        elif step:
            wake = [free[side] - FILL * 0.5 for side in range(2) if ready[side]]
            if wake and min(wake) < step[0] and min(wake) > now:
                now = min(wake)
                continue
            now = max(now, step[0]) + steps[step[1]][2]
            ended[step[1]] = now
            order.append(("step", step[1]))
            if step[1] in ("local", "ywait"):
                side = int(step[1] == "ywait")
                free[side] = max(free[side], now) + 1.0
            del steps[step[1]]
        else:
            now = max(now, min(free[side] for side in range(2) if ready[side]) - FILL * 0.5)
    return order, ended, now


def kernel(
    hidden_in, drive_in, wide_poles_in, narrow_poles_in, log_step_in, forget_in, wide_input_in, narrow_input_in,
    wide_output_in, narrow_output_in, skip_in, mix_gain_in, out_weight, mlp_gain_in, up_weight, down_weight,
    out,
    drive, wide_poles, narrow_poles, log_step, forget, wide_input, narrow_input,
    wide_output, narrow_output, skip, mix_gain, mlp_gain,
    up_a, up_b, dn_a, dn_b, mats, normed, own_in, carried,
    push_r, push_i, decay, ymsg, zmsg, gains, act_out, act_in, squared,
    loc_sem, w_send, s1_recv, s2_recv, m_send, m_recv, ag_send, ag_recv, t_send, t_recv,
    *pieces,
):
    part, pair_in, acc, half_in, side_in, final = (pieces[n :: 6] for n in range(6))
    sp, tp = lax.axis_index("sp"), lax.axis_index("tp")
    y, z, x, core = sp % 8, sp // 8, tp // 2, tp % 2

    def along_y(step):
        return z * 8 + (y + step + 8) % 8, tp

    def along_z(step):
        return ((z + step + 8) % 8) * 8 + y, tp

    def group(step):
        return sp, (tp + step) % 8

    def along_x(step):
        return sp, ((x + step + 4) % 4) * 2 + core

    partner = (sp, 2 * x + 1 - core)

    def send(src, dst, send_sem, recv_sem, to):
        pltpu.make_async_remote_copy(
            src_ref=src, dst_ref=dst, send_sem=send_sem, recv_sem=recv_sem, device_id=to, device_id_type=MESH
        ).start()

    def held(ref, sem):
        return pltpu.make_async_remote_copy(
            src_ref=ref, dst_ref=ref, send_sem=sem, recv_sem=sem, device_id=partner, device_id_type=MESH
        )

    def arrived(dst, recv_sem):
        held(dst, recv_sem).wait_recv()

    def left(src, send_sem):
        held(src, send_sem).wait_send()

    barrier = pltpu.get_barrier_semaphore()
    for step in range(1, 8):
        for to in (along_y(step), along_z(step), group(step)):
            pl.semaphore_signal(barrier, inc=1, device_id=to, device_id_type=MESH)
    bufs = (up_a, up_b, dn_a, dn_b)

    def where_of(n):
        return (y, z, along_y, along_z) if n % 2 == 0 else (z, y, along_z, along_y)

    def shard(n, first, second):
        return bufs[n].at[second * 8 + first]

    def mod8(v):
        return (v + 8) % 8

    local = []
    for n, weight in enumerate((up_weight, up_weight, down_weight, down_weight)):
        at, line, _, _ = where_of(n)
        local.append(
            pltpu.make_async_copy(weight.at[:, pl.ds((n % 2) * 512, 512)], shard(n, at, line), loc_sem.at[n])
        )
    local.append(pltpu.make_async_copy(out_weight, mats.at[tp], loc_sem.at[4]))
    local.append(pltpu.make_async_copy(hidden_in.at[pl.ds(pl.multiple_of(tp * 48, 16), 48)], own_in, loc_sem.at[5]))
    small = (
        (drive_in, drive), (wide_poles_in, wide_poles), (narrow_poles_in, narrow_poles), (log_step_in, log_step),
        (forget_in, forget), (wide_input_in, wide_input), (narrow_input_in, narrow_input),
        (wide_output_in, wide_output), (narrow_output_in, narrow_output), (skip_in, skip),
        (mix_gain_in, mix_gain), (mlp_gain_in, mlp_gain),
    )
    fetched = [pltpu.make_async_copy(src, dst, loc_sem.at[6 + n]) for n, (src, dst) in enumerate(small)]
    for copy in local[:4] + fetched + local[4:]:
        copy.start()
    def first_send(n, hop):
        at, line, go, _ = where_of(n)
        for direction in (1, -1) if hop < 4 else (1,):
            ref = shard(n, mod8(at - direction * (hop - 1)), line)
            send(ref, ref, w_send.at[n], s1_recv.at[n, hop - 1], go(direction))

    def line_send(n, s, hop):
        at, line, _, go = where_of(n)
        for k in GROUPS[s]:
            for direction in (1, -1):
                if hop < 4 or (k in RIGHTWARD) == (direction > 0):
                    ref = shard(n, mod8(at + OFFSETS[k]), mod8(line - direction * (hop - 1)))
                    send(ref, ref, w_send.at[n], s2_recv.at[n, 4 * s + hop - 1], go(direction))

    def copy_send(op):
        kind, n, s, hop = op
        if kind == "first":
            first_send(n, hop)
        else:
            line_send(n, s, hop)

    def copy_wait(op):
        kind, n, s, hop = op
        sem = s1_recv.at[n, hop - 1] if kind == "first" else s2_recv.at[n, 4 * s + hop - 1]
        count = (2 if hop < 4 else 1) * (1 if kind == "first" else len(GROUPS[s]))
        arrived(bufs[n].at[pl.ds(0, count)], sem)

    halves = (pl.ds(0, 1024), pl.ds(1024, 1024))

    def gather_start(buf, g):
        ref = buf.at[tp]
        for turn in range(2):
            for n, direction in enumerate((1, -1)):
                half = (n + turn) % 2
                piece = ref.at[:, halves[half]]
                send(piece, piece, ag_send.at[g], ag_recv.at[g, 2 * n + turn], along_x(direction))
        send(ref, ref, ag_send.at[g], ag_recv.at[g, 6], partner)

    def gather_middle(buf, g, turns=(0, 1)):
        for turn in turns:
            for n, direction in enumerate((1, -1)):
                half = (n + turn) % 2
                piece = buf.at[along_x(-direction)[1], :, halves[half]]
                arrived(piece, ag_recv.at[g, 2 * n + turn])
                if turn == 0:
                    send(piece, piece, ag_send.at[g], ag_recv.at[g, 4 + n], along_x(direction))
                send(piece, piece, ag_send.at[g], ag_recv.at[g, 6], partner)

    def gather_end(buf, g):
        far = buf.at[along_x(2)[1]]
        for n in range(2):
            piece = far.at[:, halves[n]]
            arrived(piece, ag_recv.at[g, 4 + n])
            send(piece, piece, ag_send.at[g], ag_recv.at[g, 6], partner)

    def gather_partner(buf, g):
        arrived(buf.at[pl.ds(0, 4)], ag_recv.at[g, 6])

    def message(buf, at, state, fade):
        buf[at] = jnp.concatenate([state[0], state[1], fade, fade], axis=0)

    for copy in local[:4]:
        copy.wait()
    pl.semaphore_wait(barrier, 21)
    held_values = {}

    def do_local():
        for copy in fetched + local[4:]:
            copy.wait()
        pick = order()
        decay[...] = decay_rows(forget, pick)
        drive_now = jnp.dot(pick, drive[...], preferred_element_type=F32).astype(BF)
        base, coef = discretize(wide_poles, narrow_poles, log_step)
        weights = [b.astype(BF) for b in blocks(wide_input, narrow_input)]
        pushed = times(coef, [jnp.dot(drive_now, w, preferred_element_type=F32) for w in weights])
        push_r[...] = pushed[0]
        push_i[...] = pushed[1]
        wide_base = [jnp.broadcast_to(b, (LANES, STATES)) for b in base]

        def scan_step(step, state):
            rows = pl.ds(pl.multiple_of(step * LANES, LANES), LANES)
            fade = decay[rows]
            grown = times(wide_base, state[:2])
            new = fade * grown[0] + push_r[rows], fade * grown[1] + push_i[rows], fade * state[2]
            push_r[rows], push_i[rows], decay[rows] = new
            return new

        zero = jnp.zeros((LANES, STATES), F32)
        end_r, end_i, total = lax.fori_loop(0, STEPS, scan_step, (zero, zero, zero + 1.0), unroll=4)
        powers = [base]
        for _ in range(5):
            powers.append(times(powers[-1], powers[-1]))
        run_base = times(powers[5], powers[4])
        _, last = chain((zero[:1], zero[:1]), (end_r, end_i), total, run_base)
        fade_all = total[:1]
        for run in range(1, LANES):
            fade_all = fade_all * total[run : run + 1]
        device_base = run_base
        for _ in range(3):
            device_base = times(device_base, device_base)
        line_base = device_base
        for _ in range(3):
            line_base = times(line_base, line_base)


        message(ymsg, y, last, fade_all)
        for step in range(1, 8):
            send(ymsg.at[y], ymsg.at[y], m_send.at[1], m_recv.at[1], along_y(step))
        gather_start(mats, 0)
        gains[tp] = mix_gain[...]
        for step in range(1, 8):
            send(mix_gain, gains.at[tp], m_send.at[0], m_recv.at[0], group(step))
        held_values["local"] = zero, wide_base, end_r, end_i, total, run_base, device_base, line_base, drive_now

    def do_ywait():
        arrived(ymsg.at[pl.ds(0, 7)], m_recv.at[1])
        zero, _, _, _, _, _, device_base, _, _ = held_values["local"]
        zrow, onerow = zero[:1], zero[:1] + 1.0
        whole, before = (zrow, zrow), (zrow, zrow)
        whole_fade, before_fade, before_base = onerow, onerow, (onerow, zrow)
        for k in range(8):
            got = ymsg[k]
            fade = got[2:3]
            grown = times(device_base, whole)
            new = fade * grown[0] + got[0:1], fade * grown[1] + got[1:2]
            new_fade = whole_fade * fade
            new_base = times(before_base, device_base)
            earlier = k < y
            before = [jnp.where(earlier, n, o) for n, o in zip(new, before)]
            before_fade = jnp.where(earlier, new_fade, before_fade)
            before_base = [jnp.where(earlier, n, o) for n, o in zip(new_base, before_base)]
            whole, whole_fade = new, new_fade

        message(zmsg, z, whole, whole_fade)
        for step in range(1, 8):
            send(zmsg.at[z], zmsg.at[z], m_send.at[2], m_recv.at[2], along_z(step))
        held_values["before"] = before, before_fade, before_base

    def do_zwait():
        arrived(zmsg.at[pl.ds(0, 7)], m_recv.at[2])
        before, before_fade, before_base = held_values["before"]
        zero, _, _, _, _, _, _, line_base, _ = held_values["local"]
        zrow = zero[:1]
        enter = (zrow, zrow)
        for k in range(8):
            got = zmsg[k]
            grown = times(line_base, enter)
            new = got[2:3] * grown[0] + got[0:1], got[2:3] * grown[1] + got[1:2]
            enter = [jnp.where(k < z, n, o) for n, o in zip(new, enter)]
        grown = times(before_base, enter)
        enter = before_fade * grown[0] + before[0], before_fade * grown[1] + before[1]

        held_values["enter"] = enter

    def do_readout():
        enter = held_values["enter"]
        _, wide_base, end_r, end_i, total, run_base, _, _, drive_now = held_values["local"]
        starts, _ = chain(enter, (end_r, end_i), total, run_base)

        def fix_step(step, state):
            rows = pl.ds(pl.multiple_of(step * LANES, LANES), LANES)
            state = times(wide_base, state)
            push_r[rows] = push_r[rows] + decay[rows] * state[0]
            push_i[rows] = push_i[rows] + decay[rows] * state[1]
            return state

        lax.fori_loop(0, STEPS, fix_step, tuple(starts), unroll=4)
        real_block, imag_block = blocks(wide_output, narrow_output)
        response = lax.dot_general(push_r[...].astype(BF), real_block.astype(BF), NT, preferred_element_type=F32)
        response -= lax.dot_general(push_i[...].astype(BF), imag_block.astype(BF), NT, preferred_element_type=F32)
        response += skip[...] * drive_now.astype(F32)
        active = 0.5 * response * (1.0 + lax.erf(response * (0.5**0.5)))
        active = jnp.dot(back_order(), active.astype(BF), preferred_element_type=F32).astype(BF)

        act_out[...] = active.reshape(8, 48, 128)
        act_in[tp] = act_out[tp]
        for step in range(1, 8):
            to = group(step)
            send(act_out.at[to[1]], act_in.at[tp], m_send.at[3], m_recv.at[3], to)

    def do_act():
        arrived(gains.at[pl.ds(0, 7)], m_recv.at[0])
        arrived(act_in.at[pl.ds(0, 7)], m_recv.at[3])
        rows = jnp.concatenate([act_in[k] for k in range(8)], axis=1).astype(F32)
        gain = jnp.concatenate([gains[k] for k in range(8)], axis=1)
        power = jnp.sum(rows * rows, axis=1, keepdims=True) * (1.0 / 1024)
        held_values["mixed"] = (rows * lax.rsqrt(power + EPS) * gain).astype(BF)

    def do_proj():
        gather_partner(mats, 0)
        for n in range(8):
            cols = pl.ds(n * 256, 256)
            proj = jnp.dot(held_values["mixed"], mats[:, :, cols].reshape(1024, 256), preferred_element_type=F32)
            carried[:, cols] = (own_in[:, cols].astype(F32) + proj).astype(BF)
        values = carried[...].astype(F32)
        power = jnp.sum(values * values, axis=1, keepdims=True) * (1.0 / 2048)
        normed[tp] = (values * lax.rsqrt(power + EPS) * mlp_gain[...]).astype(BF)
        gather_start(normed, 1)

    def do_up():
        gather_partner(normed, 1)
        for n in range(4):
            cols = pl.ds((n % 2) * 256, 256)
            buf = bufs[n // 2]
            if n < 2:
                weight = buf[:, :, cols].reshape(2048, 256)
            else:
                weight = jnp.concatenate([buf[(s % 8) * 8 + s // 8, :, cols] for s in range(64)], axis=0)
            pre = jnp.dot(normed[...].reshape(384, 2048), weight, preferred_element_type=F32)
            pre = jnp.maximum(pre, 0.0)
            squared[:, pl.ds(n * 256, 256)] = (pre * pre).astype(BF)

    def chip(step):
        return (x + step + 4) % 4

    def halves_of(c):
        half = len(CHUNKS[c]) * 128
        return pl.ds(0, half), pl.ds(half, half)

    def unit(c, k):
        return mod8(z + OFFSETS[CHUNKS[c][k]])

    def do_product(c):
        for k in range(len(CHUNKS[c])):
            q = unit(c, k)
            first = dn_a[pl.ds(pl.multiple_of(q * 8, 8), 8)].reshape(256, 512)
            second = jnp.concatenate([dn_b[s * 8 + q] for s in range(8)], axis=0)
            piece = lax.dot_general(squared[:, :512], first, NT, preferred_element_type=F32)
            piece += lax.dot_general(squared[:, 512:], second, NT, preferred_element_type=F32)
            piece = piece.astype(BF)
            for b in range(8):
                part[c][(b % 2) * 4 + b // 2, :, pl.ds(k * 256, 256)] = piece[b * 48 : (b + 1) * 48]
        send(part[c].at[pl.ds((1 - core) * 4, 4)], pair_in[c], t_send.at[c], t_recv.at[c, 0], partner)

    def chip_sum(c, step, cols=slice(None)):
        at = chip(step)
        return part[c][core * 4 + at, :, cols].astype(F32) + pair_in[c][at, :, cols].astype(F32)

    def do_sum(c):
        arrived(pair_in[c], t_recv.at[c, 0])
        if c in DIRECT:
            for n, step in enumerate((2, 1, -1)):
                acc[c][n] = chip_sum(c, step).astype(BF)
                send(acc[c].at[n], side_in[c].at[n], t_send.at[c], t_recv.at[c, 3], along_x(step))
            return
        cut = halves_of(c)
        acc[c][0] = chip_sum(c, 2).astype(BF)
        for n, direction in enumerate((1, -1)):
            send(acc[c].at[0, :, cut[n]], half_in[c].at[n], t_send.at[c], t_recv.at[c, 1 + n], along_x(direction))
        for n, direction in enumerate((1, -1)):
            ready = cut[1 - n]
            acc[c][1 + n, :, ready] = chip_sum(c, direction, ready).astype(BF)
            send(
                acc[c].at[1 + n, :, ready], side_in[c].at[n, :, ready],
                t_send.at[c], t_recv.at[c, 3], along_x(direction),
            )

    def do_on(c):
        cut = halves_of(c)
        for n, direction in enumerate((1, -1)):
            arrived(half_in[c].at[n], t_recv.at[c, 1 + n])
            acc[c][1 + n, :, cut[n]] = (chip_sum(c, direction, cut[n]) + half_in[c][n].astype(F32)).astype(BF)
            send(
                acc[c].at[1 + n, :, cut[n]], side_in[c].at[n, :, cut[n]],
                t_send.at[c], t_recv.at[c, 3], along_x(direction),
            )

    def do_done(c):
        cols = [carried[:, pl.ds(pl.multiple_of(unit(c, k) * 256, 256), 256)] for k in range(len(CHUNKS[c]))]
        mine = chip_sum(c, 0) + jnp.concatenate(cols, axis=1).astype(F32)
        arrived(side_in[c], t_recv.at[c, 3])
        for n in range(3 if c in DIRECT else 2):
            mine += side_in[c][n].astype(F32)
        final[c][tp] = mine.astype(BF)
        ref = final[c].at[tp]
        for n, step in enumerate((1, -1, 2) if c in DIRECT else (1, -1)):
            send(ref, ref, t_send.at[c], t_recv.at[c, 4 + n], along_x(step))
        send(ref, ref, t_send.at[c], t_recv.at[c, 8], partner)

    def do_pass(c):
        for n, step in enumerate((1, -1, 2) if c in DIRECT else (1, -1)):
            ref = final[c].at[along_x(-step)[1]]
            arrived(ref, t_recv.at[c, 4 + n])
            if c not in DIRECT:
                piece = ref.at[:, halves_of(c)[n]]
                send(piece, piece, t_send.at[c], t_recv.at[c, 6 + n], along_x(step))
            send(ref, ref, t_send.at[c], t_recv.at[c, 8], partner)

    def do_last(c):
        for n in range(2):
            piece = final[c].at[along_x(2)[1], :, halves_of(c)[n]]
            arrived(piece, t_recv.at[c, 6 + n])
            send(piece, piece, t_send.at[c], t_recv.at[c, 8], partner)

    def do_out(c):
        arrived(final[c].at[pl.ds(0, 4)], t_recv.at[c, 8])
        for k in range(len(CHUNKS[c])):
            cols = pl.ds(pl.multiple_of(unit(c, k) * 256, 256), 256)
            out[:, :, cols] = final[c][:, :, pl.ds(k * 256, 256)]

    def do_clean():
        for n in range(4):
            left(bufs[n].at[pl.ds(0, 63)], w_send.at[n])
        left(gains.at[pl.ds(0, 7)], m_send.at[0])
        left(ymsg.at[pl.ds(0, 7)], m_send.at[1])
        left(zmsg.at[pl.ds(0, 7)], m_send.at[2])
        left(act_out.at[pl.ds(0, 7)], m_send.at[3])
        left(mats.at[pl.ds(0, 7)], ag_send.at[0])
        left(normed.at[pl.ds(0, 7)], ag_send.at[1])

    do = {
        "local": do_local, "ywait": do_ywait, "zwait": do_zwait, "readout": do_readout, "act": do_act, "proj": do_proj, "up": do_up,
        "clean": do_clean,
        "mats0": lambda: gather_middle(mats, 0, (0,)), "mats1": lambda: gather_middle(mats, 0, (1,)),
        "mats2": lambda: gather_end(mats, 0),
        "rows0": lambda: gather_middle(normed, 1, (0,)), "rows1": lambda: gather_middle(normed, 1, (1,)),
        "rows2": lambda: gather_end(normed, 1),
    }
    by_chunk = {
        "product": do_product, "sum": do_sum, "on": do_on, "done": do_done, "pass": do_pass, "last": do_last,
        "out": do_out,
    }
    for kind, what in plan()[0]:
        if kind == "send":
            copy_send(what)
        elif kind == "wait":
            copy_wait(what)
        else:
            if what in do:
                do[what]()
            else:
                by_chunk[what[:-1]](int(what[-1]))
    for c in range(len(CHUNKS)):
        left(part[c], t_send.at[c])


def step(*args):
    args = list(args)
    for n in (10, 11, 13):
        args[n] = args[n].reshape(1, -1)
    args[4] = args[4].T
    for n in (6, 7):
        args[n] = jnp.swapaxes(args[n], 2, 3)
    args = [pltpu.with_memory_space_constraint(a, pltpu.HBM) for a in args]
    vmem, hbm = pl.BlockSpec(memory_space=pltpu.VMEM), pl.BlockSpec(memory_space=pltpu.HBM)
    dma = pltpu.SemaphoreType.DMA
    scratch = [
        *[pltpu.VMEM(a.shape, a.dtype) for n, a in enumerate(args) if n not in (0, 12, 14, 15)],
        *[pltpu.VMEM((64, 32, 512), BF)] * 4,
        pltpu.VMEM((8, 128, 2048), BF),
        pltpu.VMEM((8, 48, 2048), BF),
        pltpu.VMEM((48, 2048), BF),
        pltpu.VMEM((48, 2048), BF),
        *[pltpu.VMEM((384, STATES), F32)] * 3,
        *[pltpu.VMEM((8, 4, STATES), F32)] * 2,
        pltpu.VMEM((8, 1, 128), F32),
        pltpu.VMEM((8, 48, 128), BF),
        pltpu.VMEM((8, 48, 128), BF),
        pltpu.VMEM((384, 1024), BF),
        dma((18,)), dma((4,)), dma((4, 4)), dma((4, 20)), dma((4,)), dma((4,)),
        dma((2,)), dma((2, 7)), dma((4,)), dma((4, 9)),
    ]
    for c, chunk in enumerate(CHUNKS):
        width = 256 * len(chunk)
        final = c in DIRECT
        scratch += [
            pltpu.VMEM((14, 48, width), BF),
            pltpu.VMEM((4, 48, width), BF),
            pltpu.VMEM((3, 48, width), BF),
            pltpu.VMEM((2, 48, width // 2), BF),
            pltpu.VMEM((3 if final else 2, 48, width), BF),
            pltpu.VMEM((8, 48, width), BF),
        ]
    whole = pl.pallas_call(
        kernel,
        out_shape=jax.ShapeDtypeStruct((8, 48, 2048), BF),
        in_specs=[hbm] * 16,
        out_specs=vmem,
        scratch_shapes=scratch,
        compiler_params=pltpu.CompilerParams(
            collective_id=0, has_side_effects=True, vmem_limit_bytes=48 * 1024 * 1024
        ),
    )(*args)
    return whole.reshape(384, 2048)


def solution(mesh):
    return jax.shard_map(
        step,
        mesh=mesh,
        in_specs=(
            P("sp", None),
            P("sp", "tp"),
            P(None, "tp", None),
            P(None, "tp", None),
            P("tp", None),
            P("tp", None, "sp"),
            P(None, "tp", None, None),
            P(None, "tp", None, None),
            P(None, "tp", None, None),
            P(None, "tp", None, None),
            P("tp"),
            P("tp"),
            P("tp", None),
            P(),
            P("sp", "tp"),
            P("sp", "tp"),
        ),
        out_specs=P("sp", None),
        check_vma=False,
    )
```
